32 devices in a mesh: sp: 8 (over z, x), tp: 4 (over y, core).
Axes of the slice: x: 2, y: 2, z: 4, core: 2. Of those that a mesh axis runs over, the one named last changes fastest.
Arguments:
- inputs: bfloat16 [4096, 4096], P('sp', 'tp'), may hold values from -6 to 6
- w_value: bfloat16 [4096, 4096], P(None, 'tp'), may hold values from -0.09375 to 0.09375
- w_gate: bfloat16 [4096, 4096], P(None, 'tp'), may hold values from -0.09375 to 0.09375
- taps: bfloat16 [31, 4096], P(None, 'tp'), may hold values from -1 to 1
- ln_gain: float32 [4096], P('tp'), may hold values from 0.1 to 1.9
- w_out: bfloat16 [4096, 4096], P(None, 'tp'), may hold values from -0.09375 to 0.09375
- grad_out: bfloat16 [4096, 4096], P('sp', 'tp'), may hold values from -6 to 6
Outputs:
- grad_input: bfloat16 [4096, 4096], P('sp', 'tp')
- grad_value_w: float32 [4096, 4096], P('sp', 'tp')
- grad_gate_w: float32 [4096, 4096], P('sp', 'tp')
- grad_out_w: float32 [4096, 4096], P('sp', 'tp')
- grad_taps: float32 [31, 4096], P(None, 'tp')
- grad_gain: float32 [4096], P('tp')
The draws below stay inside these ranges and needn't reach their ends.
All inputs are finite; a program needn't handle non-finite values.
Results may differ from the reference program's by a relative error of at most 0.017.
Values may be sent and summed in bfloat16 or wider, within the bound.
A program may use at most 128 MiB of HBM per device.

```python
import jax
import jax.numpy as jnp
from jax import lax

D = 4096
CONV = 31
SEQ = 4096
N_TP = 4


def with_spikes(result, key, source, target, shards_of, factor):
    def block_of(position):
        return (jnp.arange(result.shape[position]) // (result.shape[position] // shards_of)).reshape((-1,) + (1,) * (result.ndim - 1 - position))

    first = jax.random.permutation(key, shards_of)[block_of(target)]
    second = (block_of(target) + shards_of // 2) % shards_of
    return jnp.where((block_of(source) == first) | (block_of(source) == second), factor * result, result)


def block_scale(key, dims, cuts, low, high):
    def one(axis_at, shards_of):
        draws = jax.random.uniform(jax.random.fold_in(jax.random.fold_in(key, 6), axis_at), (shards_of,), jnp.float32, low / len(cuts), high / len(cuts))
        return jnp.repeat(jnp.exp(draws), dims[axis_at] // shards_of).reshape((-1,) + (1,) * (len(dims) - axis_at - 1))

    gain = one(*cuts[0])
    for cut in cuts[1:]:
        gain = gain * one(*cut)
    return gain


def noise(rng, shape, spread, limit, split=(), held_as=jnp.bfloat16):
    array = spread * jax.random.normal(rng, shape, jnp.float32)
    if split:
        array = array * block_scale(rng, shape, split, -0.22, 0.18)
    return jnp.clip(array, -limit, limit).astype(held_as)


def heavy_noise(own_key, extent, spread, bound, split, heavy, kind=jnp.bfloat16):
    drawn = spread * jax.random.normal(own_key, extent, jnp.float32)
    if split:
        drawn = drawn * block_scale(own_key, extent, split, -0.22, 0.18)
    return jnp.clip(with_spikes(drawn, jax.random.fold_in(own_key, 3), *heavy), -bound, bound).astype(kind)


def setup_inputs(seed: int = 0) -> dict:
    arg_keys = jax.random.split(jax.random.key(seed), 8)
    return {
        "inputs": heavy_noise(arg_keys[0], (SEQ, D), 1.0, 6.0, ((0, 8), (1, 4)), (0, 1, 8, 2.0)),
        "w_value": noise(arg_keys[1], (D, D), D ** -0.5, 0.09375, ((1, 4),)),
        "w_gate": noise(arg_keys[2], (D, D), D ** -0.5, 0.09375, ((1, 4),)),
        "taps": noise(arg_keys[3], (CONV, D), CONV ** -0.5, 1.0, ((1, 4),)),
        "ln_gain": jnp.clip(1.0 + 0.18 * jax.random.normal(arg_keys[4], (D,), jnp.float32), 0.1, 1.9),
        "w_out": noise(arg_keys[5], (D, D), D ** -0.5, 0.09375, ((1, 4),)),
        "grad_out": heavy_noise(arg_keys[6], (SEQ, D), 1.0, 6.0, ((0, 8), (1, 4)), (0, 1, 8, 2.0)),
    }


def contract_tokens(left, right):
    return lax.dot_general(left, right, (((0,), (0,)), ((), ())), preferred_element_type=jnp.float32)

def contract_channels(left, right):
    return lax.dot_general(left, right, (((1,), (1,)), ((), ())), preferred_element_type=jnp.float32)

def reference(inputs, w_value, w_gate, taps, ln_gain, w_out, grad_out):
    seq_len = inputs.shape[0]
    full_width = inputs.shape[1]
    radius = taps.shape[0] // 2
    pre_value = jnp.dot(inputs, w_value, preferred_element_type=jnp.float32)
    pre_gate = jnp.dot(inputs, w_gate, preferred_element_type=jnp.float32)
    gate_sigmoid = jax.nn.sigmoid(pre_gate)
    hidden = (pre_value * gate_sigmoid).astype(jnp.bfloat16)
    padded = jnp.pad(hidden.astype(jnp.float32), ((radius, radius), (0, 0)))
    tap_values = taps.astype(jnp.float32)
    convolved = jnp.zeros((seq_len, full_width), jnp.float32)
    for offset in range(taps.shape[0]):
        convolved = convolved + tap_values[offset] * padded[offset:offset + seq_len]
    mean = lax.optimization_barrier(jnp.sum(convolved, axis=1, keepdims=True)) / full_width
    variance = lax.optimization_barrier(jnp.sum(convolved * convolved, axis=1, keepdims=True)) / full_width - mean * mean
    inverse = lax.rsqrt(variance + 1e-06)
    normed = (convolved - mean) * inverse
    scaled = normed * ln_gain
    activated = jax.nn.silu(scaled).astype(jnp.bfloat16)
    grad_act = jnp.dot(grad_out, w_out, preferred_element_type=jnp.float32)
    sig_scaled = jax.nn.sigmoid(scaled)
    grad_scaled = grad_act * sig_scaled * (1.0 + scaled * (1.0 - sig_scaled))
    grad_gain = lax.optimization_barrier(jnp.sum(grad_scaled * normed, axis=0))
    grad_normed = grad_scaled * ln_gain
    first_sum = lax.optimization_barrier(jnp.sum(grad_normed, axis=1, keepdims=True)) / full_width
    second_sum = lax.optimization_barrier(jnp.sum(grad_normed * normed, axis=1, keepdims=True)) / full_width
    grad_conv = inverse * (grad_normed - first_sum - normed * second_sum)
    tap_rows = []
    for offset in range(taps.shape[0]):
        tap_rows.append(lax.optimization_barrier(jnp.sum(padded[offset:offset + seq_len] * grad_conv, axis=0)))
    grad_taps = jnp.stack(tap_rows, axis=0)
    grad_padded = jnp.pad(grad_conv, ((radius, radius), (0, 0)))
    grad_hidden = jnp.zeros((seq_len, full_width), jnp.float32)
    for offset in range(taps.shape[0]):
        begin = 2 * radius - offset
        grad_hidden = grad_hidden + tap_values[offset] * grad_padded[begin:begin + seq_len]
    grad_value = (grad_hidden * gate_sigmoid).astype(jnp.bfloat16)
    grad_gate = (grad_hidden * pre_value * gate_sigmoid * (1.0 - gate_sigmoid)).astype(jnp.bfloat16)
    grad_value_w = contract_tokens(inputs, grad_value)
    grad_gate_w = contract_tokens(inputs, grad_gate)
    grad_out_w = contract_tokens(grad_out, activated)
    block = full_width // N_TP
    total = jnp.zeros((seq_len, full_width), jnp.float32)
    for index in range(N_TP):
        lower = index * block
        partial_value = contract_channels(grad_value[:, lower:lower + block], w_value[:, lower:lower + block])
        partial_value = partial_value + contract_channels(grad_gate[:, lower:lower + block], w_gate[:, lower:lower + block])
        rounded = lax.optimization_barrier(partial_value.astype(jnp.bfloat16))
        total = total + rounded.astype(jnp.float32)
    grad_input = total.astype(jnp.bfloat16)
    return (grad_input, grad_value_w, grad_gate_w, grad_out_w, grad_taps, grad_gain)
```

```python
import functools

import jax
import jax.numpy as jnp
from jax import lax
from jax.experimental import pallas as pl
from jax.experimental.pallas import tpu as pltpu
from jax.sharding import Mesh, PartitionSpec as P

MESH = pl.DeviceIdType.MESH
SP = ("outer", "pair")
AXES = ("outer", "pair", "tp")
LANES = 128
PAD = 16
ROWS = 64
F32, BF16 = jnp.float32, jnp.bfloat16


def sigmoid(value):
    return 1.0 / (1.0 + jnp.exp(-value))


def dot(left, right):
    return jnp.dot(left, right, preferred_element_type=F32)


class Sends:
    def __init__(self, sems):
        self.sems, self.open = sems, []

    def start(self, src, dst, recv, device):
        copy = pltpu.make_async_remote_copy(
            src_ref=src, dst_ref=dst, send_sem=self.sems.at[len(self.open)],
            recv_sem=recv, device_id=device, device_id_type=MESH,
        )
        copy.start()
        self.open.append((copy, None))

    def start_if(self, cond, src, dst, recv, device):
        copy = pltpu.make_async_remote_copy(
            src_ref=src, dst_ref=dst, send_sem=self.sems.at[len(self.open)],
            recv_sem=recv, device_id=device, device_id_type=MESH,
        )
        pl.when(cond)(copy.start)
        self.open.append((copy, cond))

    def drain(self):
        for copy, cond in self.open:
            if cond is None:
                copy.wait_send()
            else:
                pl.when(cond)(copy.wait_send)


def arrived(ref, recv):
    pltpu.make_async_copy(ref, ref, recv).wait()


def front_kernel(
    n_outer, n_tp, conv,
    x_ref, g_ref, wv_ref, wg_ref, wo_ref, taps_ref, gain_ref,
    xg_out, gg_out, px_out, pg_out, act_out, gv_out, gt_out, small_out,
    xg, gg, wv, wg, wo, pv, ps, ga, cv, hp, gc, act, gv, gt, small,
    sum_a, sum_b, mean_b, inv_b, stat1, stat2,
    send_sems, recv_x, recv_g, recv_px, recv_pg, recv_h, recv_c, recv_s1, recv_s2, load_sems, own_sems, out_sems,
):
    outer, pair, tp = (lax.axis_index(name) for name in AXES)
    seq, n_seq, per = outer * 2 + pair, n_outer * 2, (n_outer * 2) // n_tp
    tokens, width = xg.shape[1], xg.shape[2]
    n_lane, total = pv.shape[0], width * n_seq
    sibling = tp + 1 - 2 * lax.rem(tp, 2)
    core, n_y = lax.rem(tp, 2), n_tp // 2
    across = [lax.rem(tp + 2 * step, n_tp) for step in range(1, n_y)]
    radius = conv // 2
    before, after = seq - 1, seq + 1
    has_before, has_after = seq > 0, seq < n_seq - 1
    home = lambda index: (outer, pair, index)
    beside = lambda index: (lax.div(index, 2), lax.rem(index, 2), tp)
    facing = (outer, 1 - pair, tp)

    barrier = pltpu.get_barrier_semaphore()

    def greet(device):
        pl.semaphore_signal(barrier, inc=1, device_id=device, device_id_type=MESH)

    for step in range(1, n_tp):
        greet(home(lax.rem(tp + step, n_tp)))
    pl.when(has_before)(lambda: greet(beside(before)))
    pl.when(has_after)(lambda: greet(beside(after)))
    greet(facing)

    block = lambda b, h: b * per + h
    order = [tp, sibling]
    for other in across:
        order += [other, other + 1 - 2 * core]
    loads = []
    for name, (hbm, vmem) in enumerate(((wv_ref, wv), (wg_ref, wg), (wo_ref, wo))):
        loads.append([])
        for rank, b in enumerate(order):
            for h in range(per):
                index = block(b, h)
                row = pl.multiple_of(index * width, width)
                loads[-1].append(
                    pltpu.make_async_copy(hbm.at[pl.ds(row, width), :], vmem.at[index], load_sems.at[name, rank * per + h])
                )
    owns = []
    for name, (hbm, vmem) in enumerate(((x_ref, xg), (g_ref, gg))):
        owns.append([])
        for h in range(per):
            owns[-1].append(
                pltpu.make_async_copy(hbm.at[:, pl.ds(h * width, width)], vmem.at[block(tp, h)], own_sems.at[name, h])
            )
    for copy in owns[0]:
        copy.start()
    for step in range(2 * per):
        loads[0][step].start()
        loads[1][step].start()
    for copy in owns[1]:
        copy.start()
    for step in range(2 * per):
        loads[2][step].start()
    for step in range(2 * per, n_tp * per):
        loads[0][step].start()
        loads[1][step].start()
    for step in range(2 * per, n_tp * per):
        loads[2][step].start()

    count = n_tp - 1 + 1 + has_before.astype(jnp.int32) + has_after.astype(jnp.int32)
    pl.semaphore_wait(barrier, count)

    sends = Sends(send_sems)
    for hbm, vmem, recv in ((x_ref, xg, recv_x), (g_ref, gg, recv_g)):
        for h in range(per):
            src, index = hbm.at[:, pl.ds(h * width, width)], block(tp, h)
            for other in [sibling] + across:
                sends.start(src, vmem.at[index], recv.at[index], home(other))
    crossing = pl.multiple_of((1 - pair) * width, width)
    sends.start(x_ref.at[:, pl.ds(crossing, width)], px_out.at[tp], recv_px.at[tp], facing)
    sends.start(g_ref.at[:, pl.ds(crossing, width)], pg_out.at[tp], recv_pg.at[tp], facing)

    def project(ranks, left, pairs, first):
        def body(j, carry):
            column = pl.multiple_of(j * 256, 256)
            for weight, result in pairs:
                value = None
                for rank in ranks:
                    b, h = order[rank // per], rank % per
                    index = block(b, h)
                    part = dot(left[index], weight[index, :, pl.ds(column, 256)])
                    value = part if value is None else value + part
                for half in range(2):
                    piece = value[:, half * LANES : (half + 1) * LANES]
                    if first:
                        result[2 * j + half] = piece
                    else:
                        result[2 * j + half] += piece
            return carry

        lax.fori_loop(0, n_lane // 2, body, 0)

    def ready(ranks, names):
        for rank in ranks:
            for name in names:
                loads[name][rank].wait()

    near = list(range(per))
    side = list(range(per, 2 * per))
    for copy in owns[0]:
        copy.wait()
    ready(near, (0, 1))
    project(near, xg, ((wv, pv), (wg, ps)), True)
    for rank in side:
        index = block(sibling, rank % per)
        arrived(xg.at[index], recv_x.at[index])
    ready(side, (0, 1))
    project(side, xg, ((wv, pv), (wg, ps)), False)
    for copy in owns[1]:
        copy.wait()
    for rank in side:
        index = block(sibling, rank % per)
        arrived(gg.at[index], recv_g.at[index])
    ready(near + side, (2,))
    project(near + side, gg, ((wo, ga),), True)

    def land(vmem, recv, b, h, crossed, recv_crossed):
        index = block(b, h)
        arrived(vmem.at[index], recv.at[index])
        sends.start(vmem.at[index], vmem.at[index], recv.at[index], home(sibling))
        sends.start_if(h != pair, vmem.at[index], crossed.at[b], recv_crossed.at[b], facing)

    for step, other in enumerate(across):
        for h in range(per):
            land(xg, recv_x, other, h, px_out, recv_px)
            rank = (2 + 2 * step) * per + h
            ready([rank], (0, 1))
            project([rank], xg, ((wv, pv), (wg, ps)), False)
            twin, index = rank + per, block(other + 1 - 2 * core, h)
            arrived(xg.at[index], recv_x.at[index])
            ready([twin], (0, 1))
            project([twin], xg, ((wv, pv), (wg, ps)), False)

    def gate(i, carry):
        c, r = lax.div(i, tokens // ROWS), lax.rem(i, tokens // ROWS)
        rows = pl.ds(pl.multiple_of(r * ROWS, ROWS), ROWS)
        sig = sigmoid(ps[c, rows, :])
        ps[c, rows, :] = sig
        hp[c, pl.ds(pl.multiple_of(r * ROWS + PAD, 8), ROWS), :] = (pv[c, rows, :] * sig).astype(BF16).astype(F32)
        return carry

    lax.fori_loop(0, n_lane * (tokens // ROWS), gate, 0)

    def halo(buffer, recv):
        @pl.when(jnp.logical_not(has_before))
        def _():
            buffer[:, 0:PAD, :] = jnp.zeros((n_lane, PAD, LANES), F32)

        @pl.when(jnp.logical_not(has_after))
        def _():
            buffer[:, PAD + tokens : 2 * PAD + tokens, :] = jnp.zeros((n_lane, PAD, LANES), F32)

        sends.start_if(has_after, buffer.at[:, pl.ds(tokens, PAD), :], buffer.at[:, pl.ds(0, PAD), :], recv.at[0], beside(after))
        sends.start_if(has_before, buffer.at[:, pl.ds(PAD, PAD), :], buffer.at[:, pl.ds(PAD + tokens, PAD), :], recv.at[1], beside(before))

    def halo_here(buffer, recv):
        pl.when(has_before)(lambda: arrived(buffer.at[:, pl.ds(0, PAD), :], recv.at[0]))
        pl.when(has_after)(lambda: arrived(buffer.at[:, pl.ds(PAD + tokens, PAD), :], recv.at[1]))

    halo(hp, recv_h)

    def convolve(r):
        rows = pl.ds(pl.multiple_of(r * ROWS, ROWS), ROWS)

        def lane(c, carry):
            first, second = carry
            value = jnp.zeros((ROWS, LANES), F32)
            for k in range(conv):
                value = value + taps_ref[c, k : k + 1, :] * hp[c, pl.ds(r * ROWS + (PAD + k - radius), ROWS), :]
            cv[c, rows, :] = value
            return first + value, second + value * value

        zero = jnp.zeros((ROWS, LANES), F32)
        first, second = lax.fori_loop(0, n_lane, lane, (zero, zero))
        sum_a[rows, :] = first
        sum_b[rows, :] = second

    def inner_rows(body):
        def step(r, carry):
            body(r)
            return carry

        lax.fori_loop(1, tokens // ROWS - 1, step, 0)

    inner_rows(convolve)
    halo_here(hp, recv_h)
    convolve(0)
    convolve(tokens // ROWS - 1)

    def to_row(value):
        return jnp.sum(value.T, axis=0, keepdims=True)

    def to_rows(row):
        return jnp.broadcast_to(row, (LANES, tokens)).T

    def send_sums(stat, recv):
        stat[tp, 0:1, :] = to_row(sum_a[...])
        stat[tp, 1:2, :] = to_row(sum_b[...])
        for step in range(1, n_tp):
            sends.start(stat.at[tp], stat.at[tp], recv.at[tp], home(lax.rem(tp + step, n_tp)))

    def take_sums(stat, recv):
        for step in range(1, n_tp):
            other = lax.rem(tp + step, n_tp)
            arrived(stat.at[other], recv.at[other])
        first, second = stat[0, 0:1, :], stat[0, 1:2, :]
        for other in range(1, n_tp):
            first, second = first + stat[other, 0:1, :], second + stat[other, 1:2, :]
        return first / total, second / total

    send_sums(stat1, recv_s1)

    for step, other in enumerate(across):
        for h in range(per):
            land(gg, recv_g, other, h, pg_out, recv_pg)
            rank = (2 + 2 * step) * per + h
            twin, index = rank + per, block(other + 1 - 2 * core, h)
            arrived(gg.at[index], recv_g.at[index])
            ready([rank, twin], (2,))
            project([rank, twin], gg, ((wo, ga),), False)

    mean, square = take_sums(stat1, recv_s1)
    mean_b[...] = to_rows(mean)
    inv_b[...] = to_rows(lax.rsqrt(square - mean * mean + 1e-06))
    small[:, conv : conv + 1, :] = jnp.zeros((n_lane, 1, LANES), F32)

    def backward(r, carry):
        rows = pl.ds(pl.multiple_of(r * ROWS, ROWS), ROWS)
        mean_r, inv_r = mean_b[rows, :], inv_b[rows, :]

        def lane(c, carry):
            first, second = carry
            normed = (cv[c, rows, :] - mean_r) * inv_r
            cv[c, rows, :] = normed
            gain = gain_ref[c]
            scaled = normed * gain
            sig = sigmoid(scaled)
            act[rows, pl.ds(pl.multiple_of(c * LANES, LANES), LANES)] = (scaled * sig).astype(BF16)
            grad_scaled = ga[c, rows, :] * sig * (1.0 + scaled * (1.0 - sig))
            small[c, conv : conv + 1, :] += jnp.sum(grad_scaled * normed, axis=0, keepdims=True)
            grad_normed = grad_scaled * gain
            gc[c, pl.ds(pl.multiple_of(r * ROWS + PAD, 8), ROWS), :] = grad_normed
            return first + grad_normed, second + grad_normed * normed

        zero = jnp.zeros((ROWS, LANES), F32)
        first, second = lax.fori_loop(0, n_lane, lane, (zero, zero))
        sum_a[rows, :] = first
        sum_b[rows, :] = second
        return carry

    lax.fori_loop(0, tokens // ROWS, backward, 0)
    send_sums(stat2, recv_s2)
    outs = [pltpu.make_async_copy(act, act_out, out_sems.at[0])]
    outs[0].start()
    first_mean, second_mean = take_sums(stat2, recv_s2)
    sum_a[...] = to_rows(first_mean)
    sum_b[...] = to_rows(second_mean)

    def finish(r):
        rows = pl.ds(pl.multiple_of(r * ROWS, ROWS), ROWS)
        padded = pl.ds(pl.multiple_of(r * ROWS + PAD, 8), ROWS)
        inv_r, first_r, second_r = inv_b[rows, :], sum_a[rows, :], sum_b[rows, :]

        def lane(c, carry):
            gc[c, padded, :] = inv_r * (gc[c, padded, :] - first_r - cv[c, rows, :] * second_r)
            return carry

        lax.fori_loop(0, n_lane, lane, 0)

    finish(0)
    finish(tokens // ROWS - 1)
    halo(gc, recv_c)
    inner_rows(finish)

    def spread(r):
        rows = pl.ds(pl.multiple_of(r * ROWS, ROWS), ROWS)

        def lane(c, carry):
            value = jnp.zeros((ROWS, LANES), F32)
            for k in range(conv):
                value = value + taps_ref[c, k : k + 1, :] * gc[c, pl.ds(r * ROWS + (PAD + radius - k), ROWS), :]
            sig = ps[c, rows, :]
            columns = pl.ds(pl.multiple_of(c * LANES, LANES), LANES)
            lead = value * sig
            gv[rows, columns] = lead.astype(BF16)
            gt[rows, columns] = (value * pv[c, rows, :] * sig * (1.0 - sig)).astype(BF16)
            return carry

        lax.fori_loop(0, n_lane, lane, 0)

    inner_rows(spread)
    halo_here(gc, recv_c)
    spread(0)
    spread(tokens // ROWS - 1)
    outs.append(pltpu.make_async_copy(gv, gv_out, out_sems.at[1]))
    outs.append(pltpu.make_async_copy(gt, gt_out, out_sems.at[2]))
    outs.append(pltpu.make_async_copy(xg, xg_out, out_sems.at[3]))
    outs.append(pltpu.make_async_copy(gg, gg_out, out_sems.at[4]))
    for copy in outs[1:]:
        copy.start()

    mine = [tp] + across
    for crossed, recv in ((px_out, recv_px), (pg_out, recv_pg)):
        for b in mine:
            arrived(crossed.at[b], recv.at[b])
            sends.start(crossed.at[b], crossed.at[b], recv.at[b], home(sibling))

    def tap_sums(c, carry):
        def step(r, sums):
            row = pl.multiple_of(r * 8, 8)
            grad = gc[c, pl.ds(pl.multiple_of(row + PAD, 8), 8), :]
            return tuple(sums[k] + hp[c, pl.ds(row + (PAD + k - radius), 8), :] * grad for k in range(conv))

        sums = lax.fori_loop(0, tokens // 8, step, tuple(jnp.zeros((8, LANES), F32) for _ in range(conv)))
        for k in range(conv):
            small[c, k : k + 1, :] = jnp.sum(sums[k], axis=0, keepdims=True)
        return carry

    lax.fori_loop(0, n_lane, tap_sums, 0)
    outs.append(pltpu.make_async_copy(small, small_out, out_sems.at[5]))
    outs[-1].start()
    for crossed, recv in ((px_out, recv_px), (pg_out, recv_pg)):
        for b in mine:
            twin = b + 1 - 2 * core
            arrived(crossed.at[twin], recv.at[twin])
    sends.drain()
    for copy in outs:
        copy.wait()


def front(inputs, w_value, w_gate, taps, ln_gain, w_out, grad_out):
    n_outer, n_tp = lax.axis_size("outer"), lax.axis_size("tp")
    n_seq = n_outer * 2
    tokens, own = inputs.shape
    conv, channels = taps.shape
    width = own * n_tp // n_seq
    per, n_lane, n_y = n_seq // n_tp, channels // LANES, n_tp // 2
    tap_cells = jnp.pad(taps.astype(F32), ((0, 1), (0, 0))).reshape(conv + 1, n_lane, LANES).transpose(1, 0, 2)
    gain_cells = ln_gain.reshape(n_lane, 1, LANES)
    n_sends = 2 * (per * n_y + 1 + (n_y - 1) * per * 2 + n_y) + 4 + 2 * (n_tp - 1)
    any_spec, vmem_spec = pl.BlockSpec(memory_space=pl.ANY), pl.BlockSpec(memory_space=pltpu.VMEM)
    lanes = lambda rows, dtype=F32: pltpu.VMEM((n_lane, rows, LANES), dtype)
    dma = lambda *shape: pltpu.SemaphoreType.DMA(shape)
    out_shapes = [
        ((n_seq, tokens, width), BF16), ((n_seq, tokens, width), BF16),
        ((n_tp, tokens, width), BF16), ((n_tp, tokens, width), BF16),
        ((tokens, channels), BF16), ((tokens, channels), BF16), ((tokens, channels), BF16),
        ((n_lane, conv + 1, LANES), F32),
    ]
    flops = 2 * 3 * tokens * own * n_tp * channels
    return pl.pallas_call(
        functools.partial(front_kernel, n_outer, n_tp, conv),
        name="front",
        out_shape=[jax.ShapeDtypeStruct(shape, dtype) for shape, dtype in out_shapes],
        in_specs=[any_spec] * 5 + [vmem_spec] * 2,
        out_specs=[any_spec] * len(out_shapes),
        scratch_shapes=[
            pltpu.VMEM((n_seq, tokens, width), BF16), pltpu.VMEM((n_seq, tokens, width), BF16),
            *[pltpu.VMEM((n_seq, width, channels), BF16)] * 3,
            lanes(tokens), lanes(tokens), lanes(tokens), lanes(tokens),
            lanes(tokens + 2 * PAD), lanes(tokens + 2 * PAD),
            *[pltpu.VMEM((tokens, channels), BF16)] * 3,
            lanes(conv + 1),
            *[pltpu.VMEM((tokens, LANES), F32)] * 4,
            *[pltpu.VMEM((n_tp, 8, tokens), F32)] * 2,
            dma(n_sends), dma(n_seq), dma(n_seq), dma(n_tp), dma(n_tp), dma(2), dma(2), dma(n_tp), dma(n_tp),
            dma(3, n_seq), dma(2, per), dma(6),
        ],
        compiler_params=pltpu.CompilerParams(
            collective_id=0, has_side_effects=True, vmem_limit_bytes=63 * 1024 * 1024
        ),
        cost_estimate=pl.CostEstimate(flops=flops, bytes_accessed=40 * 2**20, transcendentals=0),
    )(inputs, grad_out, w_value, w_gate, w_out, tap_cells, gain_cells)


def sum_tokens(value):
    count, step = lax.axis_size(SP), 1
    while step < count:
        value = value + lax.ppermute(value, SP, [(i, i ^ step) for i in range(count)])
        step *= 2
    return value


def swap(value):
    return lax.ppermute(value, "pair", [(0, 1), (1, 0)])


def contract_channels(left, right):
    return lax.dot_general(left, right, (((1,), (1,)), ((), ())), preferred_element_type=F32)


def contract_tokens(left, right):
    value = lax.dot_general(left, right, (((1,), (0,)), ((), ())), preferred_element_type=F32)
    return value.reshape(-1, value.shape[-1])


def scatter_rows(value):
    return lax.psum_scatter(value.astype(BF16), "outer", scatter_dimension=0, tiled=True).astype(F32)


def scatter_channels(value):
    count, me = lax.axis_size("tp"), lax.axis_index("tp")
    width = value.shape[1] // count

    def part(owner):
        return lax.dynamic_slice_in_dim(value, lax.rem(owner, count) * width, width, axis=1)

    total = part(me).astype(F32)
    for step in range(1, count):
        sent = lax.ppermute(part(me + step), "tp", [(i, (i + step) % count) for i in range(count)])
        total = total + sent.astype(F32)
    return total.astype(BF16)


def local(inputs, w_value, w_gate, taps, ln_gain, w_out, grad_out):
    xg, gg, px, pg, activated, grad_value, grad_gate, small = front(
        inputs, w_value, w_gate, taps, ln_gain, w_out, grad_out
    )
    own = lax.axis_index("pair")
    conv = taps.shape[0]

    def mine(cells):
        split = cells.reshape(cells.shape[0] // 2, 2, *cells.shape[1:])
        return lax.dynamic_index_in_dim(split, own, 1, keepdims=False)

    pair_activated = swap(activated)
    pair_value, pair_gate = swap(grad_value), swap(grad_gate)
    token_sums = sum_tokens(small.transpose(1, 0, 2).reshape(conv + 1, -1))
    grad_taps, grad_gain = token_sums[:-1], token_sums[-1]
    grad_out_w = scatter_rows(contract_tokens(mine(gg), activated) + contract_tokens(pg, pair_activated))
    grad_value_w = scatter_rows(contract_tokens(mine(xg), grad_value) + contract_tokens(px, pair_value))
    grad_gate_w = scatter_rows(contract_tokens(mine(xg), grad_gate) + contract_tokens(px, pair_gate))
    partial_value = contract_channels(grad_value, w_value) + contract_channels(grad_gate, w_gate)
    grad_input = scatter_channels(partial_value.astype(BF16))
    return (grad_input, grad_value_w, grad_gate_w, grad_out_w, grad_taps, grad_gain)


def solution(mesh):
    count, across = mesh.devices.shape
    fine = Mesh(mesh.devices.reshape(count // 2, 2, across), AXES)
    in_specs = (P(SP, "tp"), P(None, "tp"), P(None, "tp"), P(None, "tp"), P("tp"), P(None, "tp"), P(SP, "tp"))
    out_specs = (P(SP, "tp"), P(SP, "tp"), P(SP, "tp"), P(SP, "tp"), P(None, "tp"), P("tp"))
    return jax.shard_map(local, mesh=fine, in_specs=in_specs, out_specs=out_specs, check_vma=False)
```

```python
import functools

import jax
import jax.numpy as jnp
from jax import lax
from jax.experimental import pallas as pl
from jax.experimental.pallas import tpu as pltpu
from jax.sharding import Mesh, PartitionSpec as P

MESH = pl.DeviceIdType.MESH
SP = ("outer", "pair")
AXES = ("outer", "pair", "tp")
LANES = 128
PAD = 16
ROWS = 64
F32, BF16 = jnp.float32, jnp.bfloat16


def sigmoid(value):
    return 1.0 / (1.0 + jnp.exp(-value))


def dot(left, right):
    return jnp.dot(left, right, preferred_element_type=F32)


class Sends:
    def __init__(self, sems):
        self.sems, self.open = sems, []

    def start(self, src, dst, recv, device):
        copy = pltpu.make_async_remote_copy(
            src_ref=src, dst_ref=dst, send_sem=self.sems.at[len(self.open)],
            recv_sem=recv, device_id=device, device_id_type=MESH,
        )
        copy.start()
        self.open.append((copy, None))

    def start_if(self, cond, src, dst, recv, device):
        copy = pltpu.make_async_remote_copy(
            src_ref=src, dst_ref=dst, send_sem=self.sems.at[len(self.open)],
            recv_sem=recv, device_id=device, device_id_type=MESH,
        )
        pl.when(cond)(copy.start)
        self.open.append((copy, cond))

    def drain(self):
        for copy, cond in self.open:
            if cond is None:
                copy.wait_send()
            else:
                pl.when(cond)(copy.wait_send)


def arrived(ref, recv):
    pltpu.make_async_copy(ref, ref, recv).wait()


def front_kernel(
    n_outer, n_tp, conv,
    x_ref, g_ref, wv_ref, wg_ref, wo_ref, taps_ref, gain_ref,
    xg_out, gg_out, px_out, pg_out, lg_out, act_out, gv_out, gt_out, small_out,
    xg, gg, wv, wg, wo, pv, ps, ga, cv, hp, gc, act, gv, gt, small,
    sum_a, sum_b, mean_b, inv_b, stat1, stat2,
    send_sems, recv_x, recv_g, recv_px, recv_pg, recv_l, recv_h, recv_c, recv_s1, recv_s2, load_sems, own_sems, out_sems,
):
    outer, pair, tp = (lax.axis_index(name) for name in AXES)
    seq, n_seq, per = outer * 2 + pair, n_outer * 2, (n_outer * 2) // n_tp
    tokens, width = xg.shape[1], xg.shape[2]
    n_lane, total = pv.shape[0], width * n_seq
    sibling = tp + 1 - 2 * lax.rem(tp, 2)
    core, n_y = lax.rem(tp, 2), n_tp // 2
    across = [lax.rem(tp + 2 * step, n_tp) for step in range(1, n_y)]
    radius = conv // 2
    before, after = seq - 1, seq + 1
    has_before, has_after = seq > 0, seq < n_seq - 1
    home = lambda index: (outer, pair, index)
    beside = lambda index: (lax.div(index, 2), lax.rem(index, 2), tp)
    facing = (outer, 1 - pair, tp)

    barrier = pltpu.get_barrier_semaphore()

    def greet(device):
        pl.semaphore_signal(barrier, inc=1, device_id=device, device_id_type=MESH)

    for step in range(1, n_tp):
        greet(home(lax.rem(tp + step, n_tp)))
    pl.when(has_before)(lambda: greet(beside(before)))
    pl.when(has_after)(lambda: greet(beside(after)))
    greet(facing)
    level = lambda index: (index, pair, tp)
    planes = [lax.rem(outer + step, n_outer) for step in range(1, n_outer)]
    for other in planes:
        greet(level(other))

    block = lambda b, h: b * per + h
    order = [tp, sibling]
    for other in across:
        order += [other, other + 1 - 2 * core]
    loads = []
    for name, (hbm, vmem) in enumerate(((wv_ref, wv), (wg_ref, wg), (wo_ref, wo))):
        loads.append([])
        for rank, b in enumerate(order):
            for h in range(per):
                index = block(b, h)
                row = pl.multiple_of(index * width, width)
                loads[-1].append(
                    pltpu.make_async_copy(hbm.at[pl.ds(row, width), :], vmem.at[index], load_sems.at[name, rank * per + h])
                )
    owns = []
    for name, (hbm, vmem) in enumerate(((x_ref, xg), (g_ref, gg))):
        owns.append([])
        for h in range(per):
            owns[-1].append(
                pltpu.make_async_copy(hbm.at[:, pl.ds(h * width, width)], vmem.at[block(tp, h)], own_sems.at[name, h])
            )
    for copy in owns[0]:
        copy.start()
    for step in range(2 * per):
        loads[0][step].start()
        loads[1][step].start()
    for copy in owns[1]:
        copy.start()
    for step in range(2 * per):
        loads[2][step].start()
    for step in range(2 * per, n_tp * per):
        loads[0][step].start()
        loads[1][step].start()
    for step in range(2 * per, n_tp * per):
        loads[2][step].start()

    count = n_tp - 1 + 1 + n_outer - 1 + has_before.astype(jnp.int32) + has_after.astype(jnp.int32)
    pl.semaphore_wait(barrier, count)

    sends = Sends(send_sems)
    for hbm, vmem, recv in ((x_ref, xg, recv_x), (g_ref, gg, recv_g)):
        for h in range(per):
            src, index = hbm.at[:, pl.ds(h * width, width)], block(tp, h)
            for other in [sibling] + across:
                sends.start(src, vmem.at[index], recv.at[index], home(other))
    crossing = pl.multiple_of((1 - pair) * width, width)
    sends.start(x_ref.at[:, pl.ds(crossing, width)], px_out.at[tp], recv_px.at[tp], facing)
    sends.start(g_ref.at[:, pl.ds(crossing, width)], pg_out.at[tp], recv_pg.at[tp], facing)

    def project(ranks, left, pairs, first):
        def body(j, carry):
            column = pl.multiple_of(j * 256, 256)
            for weight, result in pairs:
                value = None
                for rank in ranks:
                    b, h = order[rank // per], rank % per
                    index = block(b, h)
                    part = dot(left[index], weight[index, :, pl.ds(column, 256)])
                    value = part if value is None else value + part
                for half in range(2):
                    piece = value[:, half * LANES : (half + 1) * LANES]
                    if first:
                        result[2 * j + half] = piece
                    else:
                        result[2 * j + half] += piece
            return carry

        lax.fori_loop(0, n_lane // 2, body, 0)

    def ready(ranks, names):
        for rank in ranks:
            for name in names:
                loads[name][rank].wait()

    near = list(range(per))
    side = list(range(per, 2 * per))
    for copy in owns[0]:
        copy.wait()
    ready(near, (0, 1))
    project(near, xg, ((wv, pv), (wg, ps)), True)
    for rank in side:
        index = block(sibling, rank % per)
        arrived(xg.at[index], recv_x.at[index])
    ready(side, (0, 1))
    project(side, xg, ((wv, pv), (wg, ps)), False)
    for copy in owns[1]:
        copy.wait()
    for rank in side:
        index = block(sibling, rank % per)
        arrived(gg.at[index], recv_g.at[index])
    ready(near + side, (2,))
    project(near + side, gg, ((wo, ga),), True)

    def land(vmem, recv, b, h, crossed, recv_crossed):
        index = block(b, h)
        arrived(vmem.at[index], recv.at[index])
        sends.start(vmem.at[index], vmem.at[index], recv.at[index], home(sibling))
        sends.start_if(h != pair, vmem.at[index], crossed.at[b], recv_crossed.at[b], facing)

    for step, other in enumerate(across):
        for h in range(per):
            land(xg, recv_x, other, h, px_out, recv_px)
            rank = (2 + 2 * step) * per + h
            ready([rank], (0, 1))
            project([rank], xg, ((wv, pv), (wg, ps)), False)
            twin, index = rank + per, block(other + 1 - 2 * core, h)
            arrived(xg.at[index], recv_x.at[index])
            ready([twin], (0, 1))
            project([twin], xg, ((wv, pv), (wg, ps)), False)

    for other in planes:
        sends.start(xg.at[other * 2 + core], lg_out.at[outer, core], recv_l.at[outer, core], level(other))

    def gate(i, carry):
        c, r = lax.div(i, tokens // ROWS), lax.rem(i, tokens // ROWS)
        rows = pl.ds(pl.multiple_of(r * ROWS, ROWS), ROWS)
        sig = sigmoid(ps[c, rows, :])
        ps[c, rows, :] = sig
        hp[c, pl.ds(pl.multiple_of(r * ROWS + PAD, 8), ROWS), :] = (pv[c, rows, :] * sig).astype(BF16).astype(F32)
        return carry

    lax.fori_loop(0, n_lane * (tokens // ROWS), gate, 0)

    def halo(buffer, recv):
        @pl.when(jnp.logical_not(has_before))
        def _():
            buffer[:, 0:PAD, :] = jnp.zeros((n_lane, PAD, LANES), F32)

        @pl.when(jnp.logical_not(has_after))
        def _():
            buffer[:, PAD + tokens : 2 * PAD + tokens, :] = jnp.zeros((n_lane, PAD, LANES), F32)

        sends.start_if(has_after, buffer.at[:, pl.ds(tokens, PAD), :], buffer.at[:, pl.ds(0, PAD), :], recv.at[0], beside(after))
        sends.start_if(has_before, buffer.at[:, pl.ds(PAD, PAD), :], buffer.at[:, pl.ds(PAD + tokens, PAD), :], recv.at[1], beside(before))

    def halo_here(buffer, recv):
        pl.when(has_before)(lambda: arrived(buffer.at[:, pl.ds(0, PAD), :], recv.at[0]))
        pl.when(has_after)(lambda: arrived(buffer.at[:, pl.ds(PAD + tokens, PAD), :], recv.at[1]))

    halo(hp, recv_h)

    def convolve(r):
        rows = pl.ds(pl.multiple_of(r * ROWS, ROWS), ROWS)

        def lane(c, carry):
            first, second = carry
            value = jnp.zeros((ROWS, LANES), F32)
            for k in range(conv):
                value = value + taps_ref[c, k : k + 1, :] * hp[c, pl.ds(r * ROWS + (PAD + k - radius), ROWS), :]
            cv[c, rows, :] = value
            return first + value, second + value * value

        zero = jnp.zeros((ROWS, LANES), F32)
        first, second = lax.fori_loop(0, n_lane, lane, (zero, zero))
        sum_a[rows, :] = first
        sum_b[rows, :] = second

    def inner_rows(body):
        def step(r, carry):
            body(r)
            return carry

        lax.fori_loop(1, tokens // ROWS - 1, step, 0)

    inner_rows(convolve)
    halo_here(hp, recv_h)
    convolve(0)
    convolve(tokens // ROWS - 1)

    def to_row(value):
        return jnp.sum(value.T, axis=0, keepdims=True)

    def to_rows(row):
        return jnp.broadcast_to(row, (LANES, tokens)).T

    def send_sums(stat, recv):
        stat[tp, 0:1, :] = to_row(sum_a[...])
        stat[tp, 1:2, :] = to_row(sum_b[...])
        for step in range(1, n_tp):
            sends.start(stat.at[tp], stat.at[tp], recv.at[tp], home(lax.rem(tp + step, n_tp)))

    def take_sums(stat, recv):
        for step in range(1, n_tp):
            other = lax.rem(tp + step, n_tp)
            arrived(stat.at[other], recv.at[other])
        first, second = stat[0, 0:1, :], stat[0, 1:2, :]
        for other in range(1, n_tp):
            first, second = first + stat[other, 0:1, :], second + stat[other, 1:2, :]
        return first / total, second / total

    send_sums(stat1, recv_s1)

    for step, other in enumerate(across):
        for h in range(per):
            land(gg, recv_g, other, h, pg_out, recv_pg)
            rank = (2 + 2 * step) * per + h
            twin, index = rank + per, block(other + 1 - 2 * core, h)
            arrived(gg.at[index], recv_g.at[index])
            ready([rank, twin], (2,))
            project([rank, twin], gg, ((wo, ga),), False)

    mean, square = take_sums(stat1, recv_s1)
    mean_b[...] = to_rows(mean)
    inv_b[...] = to_rows(lax.rsqrt(square - mean * mean + 1e-06))
    small[:, conv : conv + 1, :] = jnp.zeros((n_lane, 1, LANES), F32)

    def backward(r, carry):
        rows = pl.ds(pl.multiple_of(r * ROWS, ROWS), ROWS)
        mean_r, inv_r = mean_b[rows, :], inv_b[rows, :]

        def lane(c, carry):
            first, second = carry
            normed = (cv[c, rows, :] - mean_r) * inv_r
            cv[c, rows, :] = normed
            gain = gain_ref[c]
            scaled = normed * gain
            sig = sigmoid(scaled)
            act[rows, pl.ds(pl.multiple_of(c * LANES, LANES), LANES)] = (scaled * sig).astype(BF16)
            grad_scaled = ga[c, rows, :] * sig * (1.0 + scaled * (1.0 - sig))
            small[c, conv : conv + 1, :] += jnp.sum(grad_scaled * normed, axis=0, keepdims=True)
            grad_normed = grad_scaled * gain
            gc[c, pl.ds(pl.multiple_of(r * ROWS + PAD, 8), ROWS), :] = grad_normed
            return first + grad_normed, second + grad_normed * normed

        zero = jnp.zeros((ROWS, LANES), F32)
        first, second = lax.fori_loop(0, n_lane, lane, (zero, zero))
        sum_a[rows, :] = first
        sum_b[rows, :] = second
        return carry

    lax.fori_loop(0, tokens // ROWS, backward, 0)
    send_sums(stat2, recv_s2)
    outs = [pltpu.make_async_copy(act, act_out, out_sems.at[0])]
    outs[0].start()
    first_mean, second_mean = take_sums(stat2, recv_s2)
    sum_a[...] = to_rows(first_mean)
    sum_b[...] = to_rows(second_mean)

    def finish(r):
        rows = pl.ds(pl.multiple_of(r * ROWS, ROWS), ROWS)
        padded = pl.ds(pl.multiple_of(r * ROWS + PAD, 8), ROWS)
        inv_r, first_r, second_r = inv_b[rows, :], sum_a[rows, :], sum_b[rows, :]

        def lane(c, carry):
            gc[c, padded, :] = inv_r * (gc[c, padded, :] - first_r - cv[c, rows, :] * second_r)
            return carry

        lax.fori_loop(0, n_lane, lane, 0)

    finish(0)
    finish(tokens // ROWS - 1)
    halo(gc, recv_c)
    inner_rows(finish)

    def spread(r):
        rows = pl.ds(pl.multiple_of(r * ROWS, ROWS), ROWS)

        def lane(c, carry):
            value = jnp.zeros((ROWS, LANES), F32)
            for k in range(conv):
                value = value + taps_ref[c, k : k + 1, :] * gc[c, pl.ds(r * ROWS + (PAD + radius - k), ROWS), :]
            sig = ps[c, rows, :]
            columns = pl.ds(pl.multiple_of(c * LANES, LANES), LANES)
            lead = value * sig
            gv[rows, columns] = lead.astype(BF16)
            gt[rows, columns] = (value * pv[c, rows, :] * sig * (1.0 - sig)).astype(BF16)
            return carry

        lax.fori_loop(0, n_lane, lane, 0)

    inner_rows(spread)
    halo_here(gc, recv_c)
    spread(0)
    spread(tokens // ROWS - 1)
    outs.append(pltpu.make_async_copy(gv, gv_out, out_sems.at[1]))
    outs.append(pltpu.make_async_copy(gt, gt_out, out_sems.at[2]))
    outs.append(pltpu.make_async_copy(xg, xg_out, out_sems.at[3]))
    outs.append(pltpu.make_async_copy(gg, gg_out, out_sems.at[4]))
    for copy in outs[1:]:
        copy.start()

    for other in planes:
        arrived(lg_out.at[other, core], recv_l.at[other, core])
        sends.start(lg_out.at[other, core], lg_out.at[other, core], recv_l.at[other, core], home(sibling))
    own_lefts = [pltpu.make_async_copy(xg.at[outer * 2 + h], lg_out.at[outer, h], out_sems.at[6 + h]) for h in range(2)]
    for copy in own_lefts:
        copy.start()
    outs += own_lefts

    mine = [tp] + across
    for crossed, recv in ((px_out, recv_px), (pg_out, recv_pg)):
        for b in mine:
            arrived(crossed.at[b], recv.at[b])
            sends.start(crossed.at[b], crossed.at[b], recv.at[b], home(sibling))

    def tap_sums(c, carry):
        def step(r, sums):
            row = pl.multiple_of(r * 8, 8)
            grad = gc[c, pl.ds(pl.multiple_of(row + PAD, 8), 8), :]
            return tuple(sums[k] + hp[c, pl.ds(row + (PAD + k - radius), 8), :] * grad for k in range(conv))

        sums = lax.fori_loop(0, tokens // 8, step, tuple(jnp.zeros((8, LANES), F32) for _ in range(conv)))
        for k in range(conv):
            small[c, k : k + 1, :] = jnp.sum(sums[k], axis=0, keepdims=True)
        return carry

    lax.fori_loop(0, n_lane, tap_sums, 0)
    outs.append(pltpu.make_async_copy(small, small_out, out_sems.at[5]))
    outs[-1].start()
    for crossed, recv in ((px_out, recv_px), (pg_out, recv_pg)):
        for b in mine:
            twin = b + 1 - 2 * core
            arrived(crossed.at[twin], recv.at[twin])
    for other in planes:
        arrived(lg_out.at[other, 1 - core], recv_l.at[other, 1 - core])
    sends.drain()
    for copy in outs:
        copy.wait()


def front(inputs, w_value, w_gate, taps, ln_gain, w_out, grad_out):
    n_outer, n_tp = lax.axis_size("outer"), lax.axis_size("tp")
    n_seq = n_outer * 2
    tokens, own = inputs.shape
    conv, channels = taps.shape
    width = own * n_tp // n_seq
    per, n_lane, n_y = n_seq // n_tp, channels // LANES, n_tp // 2
    tap_cells = jnp.pad(taps.astype(F32), ((0, 1), (0, 0))).reshape(conv + 1, n_lane, LANES).transpose(1, 0, 2)
    gain_cells = ln_gain.reshape(n_lane, 1, LANES)
    n_sends = 2 * (per * n_y + 1 + (n_y - 1) * per * 2 + n_y) + 4 + 2 * (n_tp - 1) + 2 * (n_outer - 1)
    any_spec, vmem_spec = pl.BlockSpec(memory_space=pl.ANY), pl.BlockSpec(memory_space=pltpu.VMEM)
    lanes = lambda rows, dtype=F32: pltpu.VMEM((n_lane, rows, LANES), dtype)
    dma = lambda *shape: pltpu.SemaphoreType.DMA(shape)
    out_shapes = [
        ((n_seq, tokens, width), BF16), ((n_seq, tokens, width), BF16),
        ((n_tp, tokens, width), BF16), ((n_tp, tokens, width), BF16), ((n_outer, 2, tokens, width), BF16),
        ((tokens, channels), BF16), ((tokens, channels), BF16), ((tokens, channels), BF16),
        ((n_lane, conv + 1, LANES), F32),
    ]
    flops = 2 * 3 * tokens * own * n_tp * channels
    return pl.pallas_call(
        functools.partial(front_kernel, n_outer, n_tp, conv),
        name="front",
        out_shape=[jax.ShapeDtypeStruct(shape, dtype) for shape, dtype in out_shapes],
        in_specs=[any_spec] * 5 + [vmem_spec] * 2,
        out_specs=[any_spec] * len(out_shapes),
        scratch_shapes=[
            pltpu.VMEM((n_seq, tokens, width), BF16), pltpu.VMEM((n_seq, tokens, width), BF16),
            *[pltpu.VMEM((n_seq, width, channels), BF16)] * 3,
            lanes(tokens), lanes(tokens), lanes(tokens), lanes(tokens),
            lanes(tokens + 2 * PAD), lanes(tokens + 2 * PAD),
            *[pltpu.VMEM((tokens, channels), BF16)] * 3,
            lanes(conv + 1),
            *[pltpu.VMEM((tokens, LANES), F32)] * 4,
            *[pltpu.VMEM((n_tp, 8, tokens), F32)] * 2,
            dma(n_sends), dma(n_seq), dma(n_seq), dma(n_tp), dma(n_tp), dma(n_outer, 2), dma(2), dma(2), dma(n_tp), dma(n_tp),
            dma(3, n_seq), dma(2, per), dma(8),
        ],
        compiler_params=pltpu.CompilerParams(
            collective_id=0, has_side_effects=True, vmem_limit_bytes=63 * 1024 * 1024
        ),
        cost_estimate=pl.CostEstimate(flops=flops, bytes_accessed=40 * 2**20, transcendentals=0),
    )(inputs, grad_out, w_value, w_gate, w_out, tap_cells, gain_cells)


JOBS = 3


def dot_tokens(left, right):
    return lax.dot_general(left, right, (((0,), (0,)), ((), ())), preferred_element_type=F32)


def dot_channels(left, right):
    return lax.dot_general(left, right, (((1,), (1,)), ((), ())), preferred_element_type=F32)


def loop(count, body):
    def step(index, carry):
        body(index)
        return carry

    lax.fori_loop(0, count, step, 0)


def back_kernel(
    n_outer, n_tp,
    act_ref, gv_ref, gt_ref, xg_ref, gg_ref, px_ref, pg_ref, lg_ref, wv_ref, wg_ref, small_ref,
    gi_out, gvw_out, ggw_out, gow_out, small_out,
    own_left, pair_left, line_left, ag, rs, own_right, pair_right, gv, gt, weights, gi, gi_sent, gi_total,
    racc, aacc, xacc, xs, xr, small, small_x, group, group_in, group_all, small_total,
    load_sems, left_sems, weight_sems, out_sems,
    ag_send, ag_recv, rs_send, rs_recv, xr_send, xr_recv, swap_send, swap_recv, gi_send, gi_recv,
    sx_send, sx_recv, s1_send, s1_recv, s2_send, s2_recv,
):
    z, pair, tp = (lax.axis_index(name) for name in AXES)
    n, last = n_outer, n_outer - 1
    mirror = last - z
    width, half = own_left.shape[3], own_right.shape[2]
    per = gi.shape[1]
    facing = (z, 1 - pair, tp)
    level = lambda index: (index, pair, tp)
    home = lambda index: (z, pair, index)

    barrier = pltpu.get_barrier_semaphore()

    def greet(device):
        pl.semaphore_signal(barrier, inc=1, device_id=device, device_id_type=MESH)

    greet(facing)
    for step in range(1, n):
        greet(level(lax.rem(z + step, n)))
    for step in range(1, n_tp):
        greet(home(lax.rem(tp + step, n_tp)))

    def remote(src, dst, send, recv, device):
        return pltpu.make_async_remote_copy(
            src_ref=src, dst_ref=dst, send_sem=send, recv_sem=recv, device_id=device, device_id_type=MESH
        )

    local = []

    def load(src, dst, sem):
        copy = pltpu.make_async_copy(src, dst, sem)
        copy.start()
        return copy

    def weight_copies(s, slot):
        b, h = lax.rem(tp + 1 + lax.div(s, per), n_tp), lax.rem(s, per)
        row = pl.multiple_of((b * per + h) * width, width)
        return [
            pltpu.make_async_copy(ref.at[pl.ds(row, width), :], weights.at[slot, i], weight_sems.at[slot, i])
            for i, ref in enumerate((wv_ref, wg_ref))
        ]

    lead, trail = pl.ds(0, half), pl.ds(half, half)
    cells = [
        load(gv_ref.at[:, trail], ag.at[0, z], load_sems.at[0]),
        load(gt_ref.at[:, lead], ag.at[1, z], load_sems.at[1]),
        load(gt_ref.at[:, trail], ag.at[2, z], load_sems.at[2]),
    ]
    whole = [load(gv_ref, gv, load_sems.at[3]), load(gt_ref, gt, load_sems.at[4])]
    for copy in weight_copies(0, 0):
        copy.start()
    rights = [
        load(act_ref.at[:, lead], own_right.at[0], load_sems.at[5]),
        load(act_ref.at[:, trail], own_right.at[1], load_sems.at[6]),
        load(gv_ref.at[:, lead], own_right.at[2], load_sems.at[7]),
        load(small_ref, small, load_sems.at[8]),
    ]
    lefts = []
    for d in range(n):
        lefts += [
            load(gg_ref.at[d * 2 + pair], own_left.at[0, d], left_sems.at[0, d]),
            load(xg_ref.at[d * 2 + pair], own_left.at[1, d], left_sems.at[1, d]),
            load(pg_ref.at[d], pair_left.at[0, d], left_sems.at[2, d]),
            load(px_ref.at[d], pair_left.at[1, d], left_sems.at[3, d]),
            load(lg_ref.at[d], line_left.at[d], left_sems.at[4, d]),
        ]

    pl.semaphore_wait(barrier, 1 + n - 1 + n_tp - 1)

    for copy in cells:
        copy.wait()

    def ag_right(k, j):
        return remote(ag.at[j, z - k], ag.at[j, z - k], ag_send.at[0, j, k], ag_recv.at[j, z - k], level(z + 1))

    def ag_left(k, j):
        return remote(ag.at[j, z + k], ag.at[j, z + k], ag_send.at[1, j, k], ag_recv.at[j, z + k], level(z - 1))

    for j in range(JOBS):
        pl.when(z < last)(lambda: ag_right(0, j).start())
        pl.when(z > 0)(lambda: ag_left(0, j).start())
    swaps = [
        remote(src, pair_right.at[j], swap_send.at[j], swap_recv.at[j], facing)
        for j, src in enumerate((act_ref.at[:, lead], act_ref.at[:, trail], gv_ref.at[:, lead]))
    ]
    small_swap = remote(small_ref, small_x, sx_send.at[0], sx_recv.at[0], facing)
    small_swap.start()
    for copy in swaps:
        copy.start()

    for copy in whole:
        copy.wait()
    steps = n_tp * per

    def input_step(s):
        slot = lax.rem(s, 2)

        @pl.when(s < steps - 1)
        def _():
            for copy in weight_copies(s + 1, 1 - slot):
                copy.start()

        for copy in weight_copies(s, slot):
            copy.wait()
        b, h = lax.rem(tp + 1 + lax.div(s, per), n_tp), lax.rem(s, per)
        value = (dot_channels(gv[...], weights[slot, 0]) + dot_channels(gt[...], weights[slot, 1])).astype(BF16)

        @pl.when(s < steps - per)
        def _():
            gi_sent[s] = value
            remote(gi_sent.at[s], gi.at[tp, h], gi_send.at[s], gi_recv.at[tp, h], home(b)).start()

        @pl.when(s >= steps - per)
        def _():
            gi[tp, h] = value

    loop(steps, input_step)

    for copy in rights:
        copy.wait()
    small_swap.wait_recv()
    rows = group.shape[2]
    for g in range(n):
        group[g] = small[:, g * rows : (g + 1) * rows, :] + small_x[:, g * rows : (g + 1) * rows, :]
    group_in[z] = group[z]
    for step in range(1, n):
        other = lax.rem(z + step, n)
        remote(group.at[other], group_in.at[z], s1_send.at[step], s1_recv.at[z], level(other)).start()
    for copy in lefts:
        copy.wait()
    for copy in swaps:
        copy.wait_recv()

    def partial_rows(j, d):
        tensor = lax.div(j, 2)
        return dot_tokens(own_left[tensor, d], own_right[j]) + dot_tokens(pair_left[tensor, d], pair_right[j])

    def own_rows(j):
        racc[j] = partial_rows(j, z)

    def line_rows(j, source, first):
        cells = ag[j, source]
        mine = dot_tokens(line_left[source, pair], cells)
        theirs = dot_tokens(line_left[source, 1 - pair], cells)
        if first:
            aacc[j], xacc[j] = mine, theirs
        else:
            aacc[j] += mine
            xacc[j] += theirs

    def rs_right(j, d):
        return remote(rs.at[j, d], rs.at[j, d], rs_send.at[j, d], rs_recv.at[j, d], level(z + 1))

    def rs_left(j, d):
        slot = jnp.where(d == z - 1, n, d)
        return remote(rs.at[j, d], rs.at[j, slot], rs_send.at[j, d], rs_recv.at[j, slot], level(z - 1))

    def reduce_step(j, d, waiting, copy):
        value = partial_rows(j, d)

        @pl.when(waiting)
        def _():
            arrived(rs.at[j, d], rs_recv.at[j, d])
            rs[j, d] = (value + rs[j, d].astype(F32)).astype(BF16)

        @pl.when(jnp.logical_not(waiting))
        def _():
            rs[j, d] = value.astype(BF16)

        copy(j, d).start()

    farthest = jnp.maximum(z, mirror)

    def cross(j):
        xs[j] = xacc[j].astype(BF16)
        remote(xs.at[j], xr.at[j], xr_send.at[j], xr_recv.at[j], facing).start()

    loop(JOBS, lambda j: line_rows(j, z, True))

    def period(index):
        k = index + 1

        def job(j):
            @pl.when(k <= z)
            def _():
                arrived(ag.at[j, z - k], ag_recv.at[j, z - k])
                pl.when(z < last)(lambda: ag_right(k, j).start())

            @pl.when(k <= mirror)
            def _():
                arrived(ag.at[j, z + k], ag_recv.at[j, z + k])
                pl.when(z > 0)(lambda: ag_left(k, j).start())

            @pl.when(jnp.logical_and(z < last, k > z))
            def _():
                reduce_step(j, n + z - k, z > 0, rs_right)

            @pl.when(jnp.logical_and(z > 0, k > mirror))
            def _():
                reduce_step(j, k - mirror - 1, z < last, rs_left)

            pl.when(k <= z)(lambda: line_rows(j, z - k, False))
            pl.when(k <= mirror)(lambda: line_rows(j, z + k, False))
            pl.when(k == farthest)(lambda: cross(j))

        loop(JOBS, job)

        @pl.when(index == 0)
        def _():
            for step in range(1, n):
                other = lax.rem(z + step, n)
                arrived(group_in.at[other], s1_recv.at[other])
            total = group_in[0]
            for other in range(1, n):
                total = total + group_in[other]
            group_all[z] = total
            for step in range(1, n):
                remote(group_all.at[z], group_all.at[z], s2_send.at[step], s2_recv.at[z], level(lax.rem(z + step, n))).start()
            loop(JOBS, own_rows)

    loop(last, period)

    for step in range(1, n_tp):
        other = lax.rem(tp + step, n_tp)
        for h in range(per):
            arrived(gi.at[other, h], gi_recv.at[other, h])
    for h in range(per):
        total = gi[0, h].astype(F32)
        for other in range(1, n_tp):
            total = total + gi[other, h].astype(F32)
        gi_total[:, h * width : (h + 1) * width] = total.astype(BF16)
    outs = [load(gi_total, gi_out, out_sems.at[0])]
    for step in range(1, n):
        other = lax.rem(z + step, n)
        arrived(group_all.at[other], s2_recv.at[other])
    for g in range(n):
        for c in range(small.shape[0]):
            small_total[g * rows : (g + 1) * rows, c * LANES : (c + 1) * LANES] = group_all[g, c]
    outs.append(load(small_total, small_out, out_sems.at[1]))

    results = ((gvw_out, trail), (ggw_out, lead), (ggw_out, trail))
    for j, (ref, columns) in enumerate(results):
        arrived(xr.at[j], xr_recv.at[j])
        aacc[j] += xr[j].astype(F32)
        outs.append(load(aacc.at[j], ref.at[:, columns], out_sems.at[2 + j]))
    results = ((gow_out, lead), (gow_out, trail), (gvw_out, lead))
    for j, (ref, columns) in enumerate(results):
        @pl.when(z > 0)
        def _():
            arrived(rs.at[j, z], rs_recv.at[j, z])
            racc[j] += rs[j, z].astype(F32)

        @pl.when(z < last)
        def _():
            arrived(rs.at[j, n], rs_recv.at[j, n])
            racc[j] += rs[j, n].astype(F32)

        outs.append(load(racc.at[j], ref.at[:, columns], out_sems.at[5 + j]))

    def sent(j):
        def step(k):
            pl.when(jnp.logical_and(k <= z, z < last))(lambda: ag_right(k, j).wait_send())
            pl.when(jnp.logical_and(k <= mirror, z > 0))(lambda: ag_left(k, j).wait_send())
            pl.when(k > z)(lambda: rs_right(j, k).wait_send())
            pl.when(k < z)(lambda: rs_left(j, k).wait_send())

        loop(n, step)
        remote(xs.at[j], xr.at[j], xr_send.at[j], xr_recv.at[j], facing).wait_send()

    loop(JOBS, sent)
    for copy in swaps + [small_swap]:
        copy.wait_send()
    loop(steps - per, lambda s: remote(gi_sent.at[s], gi.at[tp, 0], gi_send.at[s], gi_recv.at[tp, 0], facing).wait_send())
    for step in range(1, n):
        remote(group.at[0], group_in.at[z], s1_send.at[step], s1_recv.at[z], facing).wait_send()
        remote(group_all.at[z], group_all.at[z], s2_send.at[step], s2_recv.at[z], facing).wait_send()
    for copy in outs:
        copy.wait()


def back(act, gv, gt, xg, gg, px, pg, lg, w_value, w_gate, small):
    n, n_tp = lax.axis_size("outer"), lax.axis_size("tp")
    n_seq, tokens, width = xg.shape
    channels = act.shape[1]
    n_lane, n_small = small.shape[:2]
    per, half, rows = n_seq // n_tp, channels // 2, n_small // n
    any_spec = pl.BlockSpec(memory_space=pl.ANY)
    dma = lambda *shape: pltpu.SemaphoreType.DMA(shape)
    bf, wide = (lambda *shape: pltpu.VMEM(shape, BF16)), (lambda *shape: pltpu.VMEM(shape, F32))
    out_shapes = [((tokens, width * per), BF16)] + [((width, channels), F32)] * 3 + [((n_small, channels), F32)]
    flops = 2 * 5 * tokens * width * n_seq * channels
    return pl.pallas_call(
        functools.partial(back_kernel, n, n_tp),
        name="back",
        out_shape=[jax.ShapeDtypeStruct(shape, dtype) for shape, dtype in out_shapes],
        in_specs=[any_spec] * 11,
        out_specs=[any_spec] * len(out_shapes),
        scratch_shapes=[
            bf(2, n, tokens, width), bf(2, n, tokens, width), bf(n, 2, tokens, width),
            bf(JOBS, n, tokens, half), bf(JOBS, n + 1, width, half), bf(JOBS, tokens, half), bf(JOBS, tokens, half),
            bf(tokens, channels), bf(tokens, channels), bf(2, 2, width, channels),
            bf(n_tp, per, tokens, width), bf((n_tp - 1) * per, tokens, width), bf(tokens, width * per),
            wide(JOBS, width, half), wide(JOBS, width, half), wide(JOBS, width, half),
            bf(JOBS, width, half), bf(JOBS, width, half),
            wide(n_lane, n_small, LANES), wide(n_lane, n_small, LANES),
            *[wide(n, n_lane, rows, LANES)] * 3, wide(n_small, channels),
            dma(9), dma(5, n), dma(2, 2), dma(8),
            dma(2, JOBS, n), dma(JOBS, n), dma(JOBS, n + 1), dma(JOBS, n + 1), dma(JOBS), dma(JOBS), dma(JOBS), dma(JOBS),
            dma((n_tp - 1) * per), dma(n_tp, per),
            dma(1), dma(1), dma(n), dma(n), dma(n), dma(n),
        ],
        compiler_params=pltpu.CompilerParams(
            collective_id=1, has_side_effects=True, vmem_limit_bytes=63 * 1024 * 1024
        ),
        cost_estimate=pl.CostEstimate(flops=flops, bytes_accessed=60 * 2**20, transcendentals=0),
    )(act, gv, gt, xg, gg, px, pg, lg, w_value, w_gate, small)


def local(inputs, w_value, w_gate, taps, ln_gain, w_out, grad_out):
    xg, gg, px, pg, lg, act, gv, gt, small = front(inputs, w_value, w_gate, taps, ln_gain, w_out, grad_out)
    grad_input, grad_value_w, grad_gate_w, grad_out_w, token_sums = back(
        act, gv, gt, xg, gg, px, pg, lg, w_value, w_gate, small
    )
    return (grad_input, grad_value_w, grad_gate_w, grad_out_w, token_sums[:-1], token_sums[-1])


def solution(mesh):
    count, across = mesh.devices.shape
    fine = Mesh(mesh.devices.reshape(count // 2, 2, across), AXES)
    in_specs = (P(SP, "tp"), P(None, "tp"), P(None, "tp"), P(None, "tp"), P("tp"), P(None, "tp"), P(SP, "tp"))
    out_specs = (P(SP, "tp"), P(SP, "tp"), P(SP, "tp"), P(SP, "tp"), P(None, "tp"), P("tp"))
    return jax.shard_map(local, mesh=fine, in_specs=in_specs, out_specs=out_specs, check_vma=False)
```

```python
import functools

import jax
import jax.numpy as jnp
from jax import lax
from jax.experimental import pallas as pl
from jax.experimental.pallas import tpu as pltpu
from jax.sharding import Mesh, PartitionSpec as P

MESH = pl.DeviceIdType.MESH
SP = ("outer", "pair")
AXES = ("outer", "pair", "tp")
LANES = 128
PAD = 16
ROWS = 64
F32, BF16 = jnp.float32, jnp.bfloat16


def sigmoid(value):
    return 1.0 / (1.0 + jnp.exp(-value))


def dot(left, right):
    return jnp.dot(left, right, preferred_element_type=F32)


class Sends:
    def __init__(self, sems):
        self.sems, self.open = sems, []

    def start(self, src, dst, recv, device):
        copy = pltpu.make_async_remote_copy(
            src_ref=src, dst_ref=dst, send_sem=self.sems.at[len(self.open)],
            recv_sem=recv, device_id=device, device_id_type=MESH,
        )
        copy.start()
        self.open.append((copy, None))

    def start_if(self, cond, src, dst, recv, device):
        copy = pltpu.make_async_remote_copy(
            src_ref=src, dst_ref=dst, send_sem=self.sems.at[len(self.open)],
            recv_sem=recv, device_id=device, device_id_type=MESH,
        )
        pl.when(cond)(copy.start)
        self.open.append((copy, cond))

    def drain(self):
        for copy, cond in self.open:
            if cond is None:
                copy.wait_send()
            else:
                pl.when(cond)(copy.wait_send)


def arrived(ref, recv):
    pltpu.make_async_copy(ref, ref, recv).wait()


def front_kernel(
    n_outer, n_tp, conv,
    x_ref, g_ref, wv_ref, wg_ref, wo_ref, taps_ref, gain_ref,
    xg_out, gg_out, px_out, pg_out, lg_out, act_out, gv_out, gt_out, small_out, hp_out, gc_out,
    xg, gg, wv, wg, wo, pv, ps, ga, cv, hp, gc, act, gv, gt, small,
    sum_a, sum_b, mean_b, inv_b, stat1, stat2,
    send_sems, recv_x, recv_g, recv_px, recv_pg, recv_l, recv_h, recv_c, recv_s1, recv_s2, load_sems, own_sems, out_sems,
):
    outer, pair, tp = (lax.axis_index(name) for name in AXES)
    seq, n_seq, per = outer * 2 + pair, n_outer * 2, (n_outer * 2) // n_tp
    tokens, width = xg.shape[1], xg.shape[2]
    n_lane, total = pv.shape[0], width * n_seq
    sibling = tp + 1 - 2 * lax.rem(tp, 2)
    core, n_y = lax.rem(tp, 2), n_tp // 2
    across = [lax.rem(tp + 2 * step, n_tp) for step in range(1, n_y)]
    radius = conv // 2
    before, after = seq - 1, seq + 1
    has_before, has_after = seq > 0, seq < n_seq - 1
    home = lambda index: (outer, pair, index)
    beside = lambda index: (lax.div(index, 2), lax.rem(index, 2), tp)
    facing = (outer, 1 - pair, tp)

    barrier = pltpu.get_barrier_semaphore()

    def greet(device):
        pl.semaphore_signal(barrier, inc=1, device_id=device, device_id_type=MESH)

    for step in range(1, n_tp):
        greet(home(lax.rem(tp + step, n_tp)))
    pl.when(has_before)(lambda: greet(beside(before)))
    pl.when(has_after)(lambda: greet(beside(after)))
    greet(facing)
    level = lambda index: (index, pair, tp)
    planes = [lax.rem(outer + step, n_outer) for step in range(1, n_outer)]
    for other in planes:
        greet(level(other))

    block = lambda b, h: b * per + h
    order = [tp, sibling]
    for other in across:
        order += [other, other + 1 - 2 * core]
    loads = []
    for name, (hbm, vmem) in enumerate(((wv_ref, wv), (wg_ref, wg), (wo_ref, wo))):
        loads.append([])
        for rank, b in enumerate(order):
            for h in range(per):
                index = block(b, h)
                row = pl.multiple_of(index * width, width)
                loads[-1].append(
                    pltpu.make_async_copy(hbm.at[pl.ds(row, width), :], vmem.at[index], load_sems.at[name, rank * per + h])
                )
    owns = []
    for name, (hbm, vmem) in enumerate(((x_ref, xg), (g_ref, gg))):
        owns.append([])
        for h in range(per):
            owns[-1].append(
                pltpu.make_async_copy(hbm.at[:, pl.ds(h * width, width)], vmem.at[block(tp, h)], own_sems.at[name, h])
            )
    for copy in owns[0]:
        copy.start()
    for step in range(2 * per):
        loads[0][step].start()
        loads[1][step].start()
    for copy in owns[1]:
        copy.start()
    for step in range(2 * per):
        loads[2][step].start()
    for step in range(2 * per, n_tp * per):
        loads[0][step].start()
        loads[1][step].start()
    for step in range(2 * per, n_tp * per):
        loads[2][step].start()

    count = n_tp - 1 + 1 + n_outer - 1 + has_before.astype(jnp.int32) + has_after.astype(jnp.int32)
    pl.semaphore_wait(barrier, count)

    sends = Sends(send_sems)
    for hbm, vmem, recv in ((x_ref, xg, recv_x), (g_ref, gg, recv_g)):
        for h in range(per):
            src, index = hbm.at[:, pl.ds(h * width, width)], block(tp, h)
            for other in [sibling] + across:
                sends.start(src, vmem.at[index], recv.at[index], home(other))
    crossing = pl.multiple_of((1 - pair) * width, width)
    sends.start(x_ref.at[:, pl.ds(crossing, width)], px_out.at[tp], recv_px.at[tp], facing)
    sends.start(g_ref.at[:, pl.ds(crossing, width)], pg_out.at[tp], recv_pg.at[tp], facing)

    part, n_part = lax.div(tp, 2), tokens // n_y
    part_rows = lambda index: pl.ds(pl.multiple_of(index * n_part, n_part), n_part)

    def line_send(src, b, cond):
        sends.start_if(
            jnp.logical_and(cond, b != outer), src, lg_out.at[outer, core, part_rows(part)],
            recv_l.at[outer, core, part], level(b),
        )

    line_send(x_ref.at[part_rows(part), pl.ds(pl.multiple_of(core * width, width), width)], tp, True)

    def project(ranks, left, pairs, first):
        def body(j, carry):
            column = pl.multiple_of(j * 256, 256)
            for weight, result in pairs:
                value = None
                for rank in ranks:
                    b, h = order[rank // per], rank % per
                    index = block(b, h)
                    part = dot(left[index], weight[index, :, pl.ds(column, 256)])
                    value = part if value is None else value + part
                for half in range(2):
                    piece = value[:, half * LANES : (half + 1) * LANES]
                    if first:
                        result[2 * j + half] = piece
                    else:
                        result[2 * j + half] += piece
            return carry

        lax.fori_loop(0, n_lane // 2, body, 0)

    def ready(ranks, names):
        for rank in ranks:
            for name in names:
                loads[name][rank].wait()

    near = list(range(per))
    side = list(range(per, 2 * per))
    for copy in owns[0]:
        copy.wait()
    ready(near, (0, 1))
    project(near, xg, ((wv, pv), (wg, ps)), True)
    for rank in side:
        index = block(sibling, rank % per)
        arrived(xg.at[index], recv_x.at[index])
    line_send(xg.at[block(sibling, core), part_rows(part)], sibling, True)
    ready(side, (0, 1))
    project(side, xg, ((wv, pv), (wg, ps)), False)
    for copy in owns[1]:
        copy.wait()
    for rank in side:
        index = block(sibling, rank % per)
        arrived(gg.at[index], recv_g.at[index])
    ready(near + side, (2,))
    project(near + side, gg, ((wo, ga),), True)

    def land(vmem, recv, b, h, crossed, recv_crossed):
        index = block(b, h)
        arrived(vmem.at[index], recv.at[index])
        sends.start(vmem.at[index], vmem.at[index], recv.at[index], home(sibling))
        sends.start_if(h != pair, vmem.at[index], crossed.at[b], recv_crossed.at[b], facing)

    for step, other in enumerate(across):
        for h in range(per):
            land(xg, recv_x, other, h, px_out, recv_px)
            line_send(xg.at[block(other, h), part_rows(part)], other, core == h)
            rank = (2 + 2 * step) * per + h
            ready([rank], (0, 1))
            project([rank], xg, ((wv, pv), (wg, ps)), False)
            twin, index = rank + per, block(other + 1 - 2 * core, h)
            arrived(xg.at[index], recv_x.at[index])
            line_send(xg.at[index, part_rows(part)], other + 1 - 2 * core, core == h)
            ready([twin], (0, 1))
            project([twin], xg, ((wv, pv), (wg, ps)), False)

    def gate(i, carry):
        c, r = lax.div(i, tokens // ROWS), lax.rem(i, tokens // ROWS)
        rows = pl.ds(pl.multiple_of(r * ROWS, ROWS), ROWS)
        sig = sigmoid(ps[c, rows, :])
        ps[c, rows, :] = sig
        hp[c, pl.ds(pl.multiple_of(r * ROWS + PAD, 8), ROWS), :] = (pv[c, rows, :] * sig).astype(BF16).astype(F32)
        return carry

    lax.fori_loop(0, n_lane * (tokens // ROWS), gate, 0)

    def halo(buffer, recv):
        @pl.when(jnp.logical_not(has_before))
        def _():
            buffer[:, 0:PAD, :] = jnp.zeros((n_lane, PAD, LANES), F32)

        @pl.when(jnp.logical_not(has_after))
        def _():
            buffer[:, PAD + tokens : 2 * PAD + tokens, :] = jnp.zeros((n_lane, PAD, LANES), F32)

        sends.start_if(has_after, buffer.at[:, pl.ds(tokens, PAD), :], buffer.at[:, pl.ds(0, PAD), :], recv.at[0], beside(after))
        sends.start_if(has_before, buffer.at[:, pl.ds(PAD, PAD), :], buffer.at[:, pl.ds(PAD + tokens, PAD), :], recv.at[1], beside(before))

    def halo_here(buffer, recv):
        pl.when(has_before)(lambda: arrived(buffer.at[:, pl.ds(0, PAD), :], recv.at[0]))
        pl.when(has_after)(lambda: arrived(buffer.at[:, pl.ds(PAD + tokens, PAD), :], recv.at[1]))

    halo(hp, recv_h)

    def convolve(r):
        rows = pl.ds(pl.multiple_of(r * ROWS, ROWS), ROWS)

        def lane(c, carry):
            first, second = carry
            value = jnp.zeros((ROWS, LANES), F32)
            for k in range(conv):
                value = value + taps_ref[c, k : k + 1, :] * hp[c, pl.ds(r * ROWS + (PAD + k - radius), ROWS), :]
            cv[c, rows, :] = value
            return first + value, second + value * value

        zero = jnp.zeros((ROWS, LANES), F32)
        first, second = lax.fori_loop(0, n_lane, lane, (zero, zero))
        sum_a[rows, :] = first
        sum_b[rows, :] = second

    def inner_rows(body):
        def step(r, carry):
            body(r)
            return carry

        lax.fori_loop(1, tokens // ROWS - 1, step, 0)

    inner_rows(convolve)
    halo_here(hp, recv_h)
    convolve(0)
    convolve(tokens // ROWS - 1)

    def to_row(value):
        return jnp.sum(value.T, axis=0, keepdims=True)

    def to_rows(row):
        return jnp.broadcast_to(row, (LANES, tokens)).T

    def send_sums(stat, recv):
        stat[tp, 0:1, :] = to_row(sum_a[...])
        stat[tp, 1:2, :] = to_row(sum_b[...])
        for step in range(1, n_tp):
            sends.start(stat.at[tp], stat.at[tp], recv.at[tp], home(lax.rem(tp + step, n_tp)))

    def take_sums(stat, recv):
        for step in range(1, n_tp):
            other = lax.rem(tp + step, n_tp)
            arrived(stat.at[other], recv.at[other])
        first, second = stat[0, 0:1, :], stat[0, 1:2, :]
        for other in range(1, n_tp):
            first, second = first + stat[other, 0:1, :], second + stat[other, 1:2, :]
        return first / total, second / total

    send_sums(stat1, recv_s1)

    for step, other in enumerate(across):
        for h in range(per):
            land(gg, recv_g, other, h, pg_out, recv_pg)
            rank = (2 + 2 * step) * per + h
            twin, index = rank + per, block(other + 1 - 2 * core, h)
            arrived(gg.at[index], recv_g.at[index])
            ready([rank, twin], (2,))
            project([rank, twin], gg, ((wo, ga),), False)

    mean, square = take_sums(stat1, recv_s1)
    mean_b[...] = to_rows(mean)
    inv_b[...] = to_rows(lax.rsqrt(square - mean * mean + 1e-06))
    small[:, conv : conv + 1, :] = jnp.zeros((n_lane, 1, LANES), F32)

    def backward(r, carry):
        rows = pl.ds(pl.multiple_of(r * ROWS, ROWS), ROWS)
        mean_r, inv_r = mean_b[rows, :], inv_b[rows, :]

        def lane(c, carry):
            first, second = carry
            normed = (cv[c, rows, :] - mean_r) * inv_r
            cv[c, rows, :] = normed
            gain = gain_ref[c]
            scaled = normed * gain
            sig = sigmoid(scaled)
            act[rows, pl.ds(pl.multiple_of(c * LANES, LANES), LANES)] = (scaled * sig).astype(BF16)
            grad_scaled = ga[c, rows, :] * sig * (1.0 + scaled * (1.0 - sig))
            small[c, conv : conv + 1, :] += jnp.sum(grad_scaled * normed, axis=0, keepdims=True)
            grad_normed = grad_scaled * gain
            gc[c, pl.ds(pl.multiple_of(r * ROWS + PAD, 8), ROWS), :] = grad_normed
            return first + grad_normed, second + grad_normed * normed

        zero = jnp.zeros((ROWS, LANES), F32)
        first, second = lax.fori_loop(0, n_lane, lane, (zero, zero))
        sum_a[rows, :] = first
        sum_b[rows, :] = second
        return carry

    lax.fori_loop(0, tokens // ROWS, backward, 0)
    send_sums(stat2, recv_s2)
    outs = [pltpu.make_async_copy(act, act_out, out_sems.at[0])]
    outs[0].start()

    def line_here(source, h, piece):
        ref = lg_out.at[source, h, part_rows(piece)]
        arrived(ref, recv_l.at[source, h, piece])
        return ref

    for source in planes:
        ref = line_here(source, core, part)
        for other in across + [sibling]:
            sends.start(ref, ref, recv_l.at[source, core, part], home(other))
    first_mean, second_mean = take_sums(stat2, recv_s2)
    sum_a[...] = to_rows(first_mean)
    sum_b[...] = to_rows(second_mean)

    def finish(r):
        rows = pl.ds(pl.multiple_of(r * ROWS, ROWS), ROWS)
        padded = pl.ds(pl.multiple_of(r * ROWS + PAD, 8), ROWS)
        inv_r, first_r, second_r = inv_b[rows, :], sum_a[rows, :], sum_b[rows, :]

        def lane(c, carry):
            gc[c, padded, :] = inv_r * (gc[c, padded, :] - first_r - cv[c, rows, :] * second_r)
            return carry

        lax.fori_loop(0, n_lane, lane, 0)

    finish(0)
    finish(tokens // ROWS - 1)
    halo(gc, recv_c)
    inner_rows(finish)

    def spread(r):
        rows = pl.ds(pl.multiple_of(r * ROWS, ROWS), ROWS)

        def lane(c, carry):
            value = jnp.zeros((ROWS, LANES), F32)
            for k in range(conv):
                value = value + taps_ref[c, k : k + 1, :] * gc[c, pl.ds(r * ROWS + (PAD + radius - k), ROWS), :]
            sig = ps[c, rows, :]
            columns = pl.ds(pl.multiple_of(c * LANES, LANES), LANES)
            lead = value * sig
            gv[rows, columns] = lead.astype(BF16)
            gt[rows, columns] = (value * pv[c, rows, :] * sig * (1.0 - sig)).astype(BF16)
            return carry

        lax.fori_loop(0, n_lane, lane, 0)

    inner_rows(spread)
    halo_here(gc, recv_c)
    spread(0)
    spread(tokens // ROWS - 1)
    outs.append(pltpu.make_async_copy(gv, gv_out, out_sems.at[1]))
    outs.append(pltpu.make_async_copy(gt, gt_out, out_sems.at[2]))
    outs.append(pltpu.make_async_copy(xg, xg_out, out_sems.at[3]))
    outs.append(pltpu.make_async_copy(gg, gg_out, out_sems.at[4]))
    outs.append(pltpu.make_async_copy(hp, hp_out, out_sems.at[8]))
    outs.append(pltpu.make_async_copy(gc, gc_out, out_sems.at[9]))
    for copy in outs[1:]:
        copy.start()

    own_lefts = [pltpu.make_async_copy(xg.at[outer * 2 + h], lg_out.at[outer, h], out_sems.at[6 + h]) for h in range(2)]
    for copy in own_lefts:
        copy.start()
    outs += own_lefts

    mine = [tp] + across
    for crossed, recv in ((px_out, recv_px), (pg_out, recv_pg)):
        for b in mine:
            arrived(crossed.at[b], recv.at[b])
            sends.start(crossed.at[b], crossed.at[b], recv.at[b], home(sibling))

    outs.append(pltpu.make_async_copy(small, small_out, out_sems.at[5]))
    outs[-1].start()
    for crossed, recv in ((px_out, recv_px), (pg_out, recv_pg)):
        for b in mine:
            twin = b + 1 - 2 * core
            arrived(crossed.at[twin], recv.at[twin])
    for source in planes:
        for step in range(1, n_y):
            piece = lax.rem(part + step, n_y)
            ref = line_here(source, core, piece)
            sends.start(ref, ref, recv_l.at[source, core, piece], home(sibling))
    for source in planes:
        for piece in range(n_y):
            line_here(source, 1 - core, piece)
    sends.drain()
    for copy in outs:
        copy.wait()


def front(inputs, w_value, w_gate, taps, ln_gain, w_out, grad_out):
    n_outer, n_tp = lax.axis_size("outer"), lax.axis_size("tp")
    n_seq = n_outer * 2
    tokens, own = inputs.shape
    conv, channels = taps.shape
    width = own * n_tp // n_seq
    per, n_lane, n_y = n_seq // n_tp, channels // LANES, n_tp // 2
    tap_cells = jnp.pad(taps.astype(F32), ((0, 1), (0, 0))).reshape(conv + 1, n_lane, LANES).transpose(1, 0, 2)
    gain_cells = ln_gain.reshape(n_lane, 1, LANES)
    n_sends = 2 * (per * n_y + 1 + (n_y - 1) * per * 2 + n_y) + 4 + 2 * (n_tp - 1) + 2 + 2 * (n_y - 1) * per + (n_outer - 1) * (2 * n_y - 1)
    any_spec, vmem_spec = pl.BlockSpec(memory_space=pl.ANY), pl.BlockSpec(memory_space=pltpu.VMEM)
    lanes = lambda rows, dtype=F32: pltpu.VMEM((n_lane, rows, LANES), dtype)
    dma = lambda *shape: pltpu.SemaphoreType.DMA(shape)
    out_shapes = [
        ((n_seq, tokens, width), BF16), ((n_seq, tokens, width), BF16),
        ((n_tp, tokens, width), BF16), ((n_tp, tokens, width), BF16), ((n_outer, 2, tokens, width), BF16),
        ((tokens, channels), BF16), ((tokens, channels), BF16), ((tokens, channels), BF16),
        ((n_lane, conv + 1, LANES), F32),
        ((n_lane, tokens + 2 * PAD, LANES), F32), ((n_lane, tokens + 2 * PAD, LANES), F32),
    ]
    flops = 2 * 3 * tokens * own * n_tp * channels
    return pl.pallas_call(
        functools.partial(front_kernel, n_outer, n_tp, conv),
        name="front",
        out_shape=[jax.ShapeDtypeStruct(shape, dtype) for shape, dtype in out_shapes],
        in_specs=[any_spec] * 5 + [vmem_spec] * 2,
        out_specs=[any_spec] * len(out_shapes),
        scratch_shapes=[
            pltpu.VMEM((n_seq, tokens, width), BF16), pltpu.VMEM((n_seq, tokens, width), BF16),
            *[pltpu.VMEM((n_seq, width, channels), BF16)] * 3,
            lanes(tokens), lanes(tokens), lanes(tokens), lanes(tokens),
            lanes(tokens + 2 * PAD), lanes(tokens + 2 * PAD),
            *[pltpu.VMEM((tokens, channels), BF16)] * 3,
            lanes(conv + 1),
            *[pltpu.VMEM((tokens, LANES), F32)] * 4,
            *[pltpu.VMEM((n_tp, 8, tokens), F32)] * 2,
            dma(n_sends), dma(n_seq), dma(n_seq), dma(n_tp), dma(n_tp), dma(n_outer, 2, n_y), dma(2), dma(2), dma(n_tp), dma(n_tp),
            dma(3, n_seq), dma(2, per), dma(10),
        ],
        compiler_params=pltpu.CompilerParams(
            collective_id=0, has_side_effects=True, vmem_limit_bytes=63 * 1024 * 1024
        ),
        cost_estimate=pl.CostEstimate(flops=flops, bytes_accessed=40 * 2**20, transcendentals=0),
    )(inputs, grad_out, w_value, w_gate, w_out, tap_cells, gain_cells)


JOBS = 3


def dot_tokens(left, right):
    return lax.dot_general(left, right, (((0,), (0,)), ((), ())), preferred_element_type=F32)


def dot_channels(left, right):
    return lax.dot_general(left, right, (((1,), (1,)), ((), ())), preferred_element_type=F32)


def loop(count, body):
    def step(index, carry):
        body(index)
        return carry

    lax.fori_loop(0, count, step, 0)


def back_kernel(
    n_outer, n_tp,
    act_ref, gv_ref, gt_ref, xg_ref, gg_ref, px_ref, pg_ref, lg_ref, wv_ref, wg_ref, small_ref, hp_ref, gc_ref,
    gi_out, gvw_out, ggw_out, gow_out, taps_out, gain_out,
    own_left, pair_left, line_left, ag, rs, own_right, pair_right, gv, gt, weights, gi, gi_sent, gi_total,
    racc, aacc, xacc, xs, xr, hp, gc, small, small_x, group, group_in, group_all, taps_total, gain_total,
    load_sems, left_sems, weight_sems, out_sems,
    ag_send, ag_recv, rs_send, rs_recv, xr_send, xr_recv, swap_send, swap_recv, gi_send, gi_recv,
    sx_send, sx_recv, s1_send, s1_recv, s2_send, s2_recv,
):
    z, pair, tp = (lax.axis_index(name) for name in AXES)
    n, last = n_outer, n_outer - 1
    mirror = last - z
    width, half = own_left.shape[3], own_right.shape[2]
    per = gi.shape[1]
    facing = (z, 1 - pair, tp)
    level = lambda index: (index, pair, tp)
    home = lambda index: (z, pair, index)

    barrier = pltpu.get_barrier_semaphore()

    def greet(device):
        pl.semaphore_signal(barrier, inc=1, device_id=device, device_id_type=MESH)

    greet(facing)
    for step in range(1, n):
        greet(level(lax.rem(z + step, n)))
    for step in range(1, n_tp):
        greet(home(lax.rem(tp + step, n_tp)))

    def remote(src, dst, send, recv, device):
        return pltpu.make_async_remote_copy(
            src_ref=src, dst_ref=dst, send_sem=send, recv_sem=recv, device_id=device, device_id_type=MESH
        )

    local = []

    def load(src, dst, sem):
        copy = pltpu.make_async_copy(src, dst, sem)
        copy.start()
        return copy

    def weight_copies(s, slot):
        b, h = lax.rem(tp + 1 + lax.div(s, per), n_tp), lax.rem(s, per)
        row = pl.multiple_of((b * per + h) * width, width)
        return [
            pltpu.make_async_copy(ref.at[pl.ds(row, width), :], weights.at[slot, i], weight_sems.at[slot, i])
            for i, ref in enumerate((wv_ref, wg_ref))
        ]

    lead, trail = pl.ds(0, half), pl.ds(half, half)
    cells = [
        load(gv_ref.at[:, trail], ag.at[0, z], load_sems.at[0]),
        load(gt_ref.at[:, lead], ag.at[1, z], load_sems.at[1]),
        load(gt_ref.at[:, trail], ag.at[2, z], load_sems.at[2]),
    ]
    whole = [load(gv_ref, gv, load_sems.at[3]), load(gt_ref, gt, load_sems.at[4])]
    for copy in weight_copies(0, 0):
        copy.start()
    rights = [
        load(act_ref.at[:, lead], own_right.at[0], load_sems.at[5]),
        load(act_ref.at[:, trail], own_right.at[1], load_sems.at[6]),
        load(gv_ref.at[:, lead], own_right.at[2], load_sems.at[7]),
        load(small_ref, small, load_sems.at[8]), load(hp_ref, hp, load_sems.at[9]), load(gc_ref, gc, load_sems.at[10]),
    ]
    lefts = []
    for d in range(n):
        lefts += [
            load(gg_ref.at[d * 2 + pair], own_left.at[0, d], left_sems.at[0, d]),
            load(xg_ref.at[d * 2 + pair], own_left.at[1, d], left_sems.at[1, d]),
            load(pg_ref.at[d], pair_left.at[0, d], left_sems.at[2, d]),
            load(px_ref.at[d], pair_left.at[1, d], left_sems.at[3, d]),
            load(lg_ref.at[d], line_left.at[d], left_sems.at[4, d]),
        ]

    pl.semaphore_wait(barrier, 1 + n - 1 + n_tp - 1)

    for copy in cells:
        copy.wait()

    def ag_right(k, j):
        return remote(ag.at[j, z - k], ag.at[j, z - k], ag_send.at[0, j, k], ag_recv.at[j, z - k], level(z + 1))

    def ag_left(k, j):
        return remote(ag.at[j, z + k], ag.at[j, z + k], ag_send.at[1, j, k], ag_recv.at[j, z + k], level(z - 1))

    for j in range(JOBS):
        pl.when(z < last)(lambda: ag_right(0, j).start())
        pl.when(z > 0)(lambda: ag_left(0, j).start())
    swaps = [
        remote(src, pair_right.at[j], swap_send.at[j], swap_recv.at[j], facing)
        for j, src in enumerate((act_ref.at[:, lead], act_ref.at[:, trail], gv_ref.at[:, lead]))
    ]
    small_swap = remote(small, small_x, sx_send.at[0], sx_recv.at[0], facing)
    for copy in swaps:
        copy.start()

    for copy in whole:
        copy.wait()
    steps = n_tp * per

    def input_step(s):
        slot = lax.rem(s, 2)

        @pl.when(s < steps - 1)
        def _():
            for copy in weight_copies(s + 1, 1 - slot):
                copy.start()

        for copy in weight_copies(s, slot):
            copy.wait()
        b, h = lax.rem(tp + 1 + lax.div(s, per), n_tp), lax.rem(s, per)
        value = (dot_channels(gv[...], weights[slot, 0]) + dot_channels(gt[...], weights[slot, 1])).astype(BF16)

        @pl.when(s < steps - per)
        def _():
            gi_sent[s] = value
            remote(gi_sent.at[s], gi.at[tp, h], gi_send.at[s], gi_recv.at[tp, h], home(b)).start()

        @pl.when(s >= steps - per)
        def _():
            gi[tp, h] = value

    loop(steps, input_step)

    for copy in rights:
        copy.wait()
    n_lane, rows, conv = small.shape[0], group.shape[2], small.shape[1] - 1
    radius = conv // 2

    def tap_sums(c):
        def step(r, sums):
            row = pl.multiple_of(r * 8, 8)
            grad = gc[c, pl.ds(pl.multiple_of(row + PAD, 8), 8), :]
            return tuple(sums[k] + hp[c, pl.ds(row + (PAD + k - radius), 8), :] * grad for k in range(conv))

        zeros = tuple(jnp.zeros((8, LANES), F32) for _ in range(conv))
        sums = lax.fori_loop(0, (hp.shape[1] - 2 * PAD) // 8, step, zeros)
        for k in range(conv):
            small[c, k : k + 1, :] = jnp.sum(sums[k], axis=0, keepdims=True)

    for copy in lefts:
        copy.wait()

    def partial_rows(j, d):
        tensor = lax.div(j, 2)
        return dot_tokens(own_left[tensor, d], own_right[j]) + dot_tokens(pair_left[tensor, d], pair_right[j])

    def own_rows(j):
        racc[j] = partial_rows(j, z)

    def line_rows(j, source, first):
        cells = ag[j, source]
        mine = dot_tokens(line_left[source, pair], cells)
        theirs = dot_tokens(line_left[source, 1 - pair], cells)
        if first:
            aacc[j], xacc[j] = mine, theirs
        else:
            aacc[j] += mine
            xacc[j] += theirs

    def rs_right(j, d):
        return remote(rs.at[j, d], rs.at[j, d], rs_send.at[j, d], rs_recv.at[j, d], level(z + 1))

    def rs_left(j, d):
        slot = jnp.where(d == z - 1, n, d)
        return remote(rs.at[j, d], rs.at[j, slot], rs_send.at[j, d], rs_recv.at[j, slot], level(z - 1))

    def reduce_step(j, d, waiting, copy):
        value = partial_rows(j, d)

        @pl.when(waiting)
        def _():
            arrived(rs.at[j, d], rs_recv.at[j, d])
            rs[j, d] = (value + rs[j, d].astype(F32)).astype(BF16)

        @pl.when(jnp.logical_not(waiting))
        def _():
            rs[j, d] = value.astype(BF16)

        copy(j, d).start()

    farthest = jnp.maximum(z, mirror)

    def cross(j):
        xs[j] = xacc[j].astype(BF16)
        remote(xs.at[j], xr.at[j], xr_send.at[j], xr_recv.at[j], facing).start()

    loop(JOBS, lambda j: line_rows(j, z, True))

    def period(index):
        k = index + 1

        def job(j):
            @pl.when(k <= z)
            def _():
                arrived(ag.at[j, z - k], ag_recv.at[j, z - k])
                pl.when(z < last)(lambda: ag_right(k, j).start())

            @pl.when(k <= mirror)
            def _():
                arrived(ag.at[j, z + k], ag_recv.at[j, z + k])
                pl.when(z > 0)(lambda: ag_left(k, j).start())

            pl.when(index == 0)(lambda: arrived(pair_right.at[j], swap_recv.at[j]))

            @pl.when(jnp.logical_and(z < last, k > z))
            def _():
                reduce_step(j, n + z - k, z > 0, rs_right)

            @pl.when(jnp.logical_and(z > 0, k > mirror))
            def _():
                reduce_step(j, k - mirror - 1, z < last, rs_left)

            pl.when(k <= z)(lambda: line_rows(j, z - k, False))
            pl.when(k <= mirror)(lambda: line_rows(j, z + k, False))
            pl.when(k == farthest)(lambda: cross(j))

        loop(JOBS, job)

        @pl.when(index == 0)
        def _():
            loop(n_lane, tap_sums)
            loop(JOBS, own_rows)
            small_swap.start()

        @pl.when(index == 1)
        def _():
            small_swap.wait_recv()
            for g in range(n):
                group[g] = small[:, g * rows : (g + 1) * rows, :] + small_x[:, g * rows : (g + 1) * rows, :]
            group_in[z] = group[z]
            for step in range(1, n):
                other = lax.rem(z + step, n)
                remote(group.at[other], group_in.at[z], s1_send.at[step], s1_recv.at[z], level(other)).start()

        @pl.when(index == 2)
        def _():
            for step in range(1, n):
                other = lax.rem(z + step, n)
                arrived(group_in.at[other], s1_recv.at[other])
            total = group_in[0]
            for other in range(1, n):
                total = total + group_in[other]
            group_all[z] = total
            for step in range(1, n):
                remote(group_all.at[z], group_all.at[z], s2_send.at[step], s2_recv.at[z], level(lax.rem(z + step, n))).start()

    loop(last, period)

    for step in range(1, n_tp):
        other = lax.rem(tp + step, n_tp)
        for h in range(per):
            arrived(gi.at[other, h], gi_recv.at[other, h])
    for h in range(per):
        total = gi[0, h].astype(F32)
        for other in range(1, n_tp):
            total = total + gi[other, h].astype(F32)
        gi_total[:, h * width : (h + 1) * width] = total.astype(BF16)
    outs = [load(gi_total, gi_out, out_sems.at[0])]
    for step in range(1, n):
        other = lax.rem(z + step, n)
        arrived(group_all.at[other], s2_recv.at[other])
    for g in range(n):
        kept = min(rows, conv - g * rows)
        for c in range(n_lane):
            columns = slice(c * LANES, (c + 1) * LANES)
            taps_total[g * rows : g * rows + kept, columns] = group_all[g, c, :kept]
            if kept < rows:
                gain_total[:, columns] = group_all[g, c, kept:]
    outs.append(load(taps_total, taps_out, out_sems.at[1]))
    outs.append(load(gain_total, gain_out, out_sems.at[8]))

    results = ((gvw_out, trail), (ggw_out, lead), (ggw_out, trail))
    for j, (ref, columns) in enumerate(results):
        arrived(xr.at[j], xr_recv.at[j])
        xr[j] = (aacc[j] + xr[j].astype(F32)).astype(BF16)
        outs.append(load(xr.at[j], ref.at[:, columns], out_sems.at[2 + j]))
    results = ((gow_out, lead), (gow_out, trail), (gvw_out, lead))
    for j, (ref, columns) in enumerate(results):
        @pl.when(z > 0)
        def _():
            arrived(rs.at[j, z], rs_recv.at[j, z])
            racc[j] += rs[j, z].astype(F32)

        @pl.when(z < last)
        def _():
            arrived(rs.at[j, n], rs_recv.at[j, n])
            racc[j] += rs[j, n].astype(F32)

        rs[j, z] = racc[j].astype(BF16)
        outs.append(load(rs.at[j, z], ref.at[:, columns], out_sems.at[5 + j]))

    def sent(j):
        def step(k):
            pl.when(jnp.logical_and(k <= z, z < last))(lambda: ag_right(k, j).wait_send())
            pl.when(jnp.logical_and(k <= mirror, z > 0))(lambda: ag_left(k, j).wait_send())
            pl.when(k > z)(lambda: rs_right(j, k).wait_send())
            pl.when(k < z)(lambda: rs_left(j, k).wait_send())

        loop(n, step)
        remote(xs.at[j], xr.at[j], xr_send.at[j], xr_recv.at[j], facing).wait_send()

    loop(JOBS, sent)
    for copy in swaps + [small_swap]:
        copy.wait_send()
    loop(steps - per, lambda s: remote(gi_sent.at[s], gi.at[tp, 0], gi_send.at[s], gi_recv.at[tp, 0], facing).wait_send())
    for step in range(1, n):
        remote(group.at[0], group_in.at[z], s1_send.at[step], s1_recv.at[z], facing).wait_send()
        remote(group_all.at[z], group_all.at[z], s2_send.at[step], s2_recv.at[z], facing).wait_send()
    for copy in outs:
        copy.wait()


def back(act, gv, gt, xg, gg, px, pg, lg, w_value, w_gate, small, hp, gc):
    n, n_tp = lax.axis_size("outer"), lax.axis_size("tp")
    n_seq, tokens, width = xg.shape
    channels = act.shape[1]
    n_lane, n_small = small.shape[:2]
    per, half, rows = n_seq // n_tp, channels // 2, n_small // n
    any_spec = pl.BlockSpec(memory_space=pl.ANY)
    dma = lambda *shape: pltpu.SemaphoreType.DMA(shape)
    bf, wide = (lambda *shape: pltpu.VMEM(shape, BF16)), (lambda *shape: pltpu.VMEM(shape, F32))
    out_shapes = [((tokens, width * per), BF16)] + [((width, channels), BF16)] * 3 + [((n_small - 1, channels), F32), ((1, channels), F32)]
    flops = 2 * 5 * tokens * width * n_seq * channels
    return pl.pallas_call(
        functools.partial(back_kernel, n, n_tp),
        name="back",
        out_shape=[jax.ShapeDtypeStruct(shape, dtype) for shape, dtype in out_shapes],
        in_specs=[any_spec] * 13,
        out_specs=[any_spec] * len(out_shapes),
        scratch_shapes=[
            bf(2, n, tokens, width), bf(2, n, tokens, width), bf(n, 2, tokens, width),
            bf(JOBS, n, tokens, half), bf(JOBS, n + 1, width, half), bf(JOBS, tokens, half), bf(JOBS, tokens, half),
            bf(tokens, channels), bf(tokens, channels), bf(2, 2, width, channels),
            bf(n_tp, per, tokens, width), bf((n_tp - 1) * per, tokens, width), bf(tokens, width * per),
            wide(JOBS, width, half), wide(JOBS, width, half), wide(JOBS, width, half),
            bf(JOBS, width, half), bf(JOBS, width, half),
            wide(*hp.shape), wide(*gc.shape),
            wide(n_lane, n_small, LANES), wide(n_lane, n_small, LANES),
            *[wide(n, n_lane, rows, LANES)] * 3, wide(n_small - 1, channels), wide(1, channels),
            dma(11), dma(5, n), dma(2, 2), dma(9),
            dma(2, JOBS, n), dma(JOBS, n), dma(JOBS, n + 1), dma(JOBS, n + 1), dma(JOBS), dma(JOBS), dma(JOBS), dma(JOBS),
            dma((n_tp - 1) * per), dma(n_tp, per),
            dma(1), dma(1), dma(n), dma(n), dma(n), dma(n),
        ],
        compiler_params=pltpu.CompilerParams(
            collective_id=1, has_side_effects=True, vmem_limit_bytes=63 * 1024 * 1024
        ),
        cost_estimate=pl.CostEstimate(flops=flops, bytes_accessed=60 * 2**20, transcendentals=0),
    )(act, gv, gt, xg, gg, px, pg, lg, w_value, w_gate, small, hp, gc)


def local(inputs, w_value, w_gate, taps, ln_gain, w_out, grad_out):
    xg, gg, px, pg, lg, act, gv, gt, small, hp, gc = front(inputs, w_value, w_gate, taps, ln_gain, w_out, grad_out)
    grad_input, grad_value_w, grad_gate_w, grad_out_w, grad_taps, grad_gain = back(
        act, gv, gt, xg, gg, px, pg, lg, w_value, w_gate, small, hp, gc
    )
    weights = [value.astype(F32) for value in (grad_value_w, grad_gate_w, grad_out_w)]
    return (grad_input, *weights, grad_taps, grad_gain[0])


def solution(mesh):
    count, across = mesh.devices.shape
    fine = Mesh(mesh.devices.reshape(count // 2, 2, across), AXES)
    in_specs = (P(SP, "tp"), P(None, "tp"), P(None, "tp"), P(None, "tp"), P("tp"), P(None, "tp"), P(SP, "tp"))
    out_specs = (P(SP, "tp"), P(SP, "tp"), P(SP, "tp"), P(SP, "tp"), P(None, "tp"), P("tp"))
    return jax.shard_map(local, mesh=fine, in_specs=in_specs, out_specs=out_specs, check_vma=False)
```

```python
import functools

import jax
import jax.numpy as jnp
from jax import lax
from jax.experimental import pallas as pl
from jax.experimental.pallas import tpu as pltpu
from jax.sharding import Mesh, PartitionSpec as P

MESH = pl.DeviceIdType.MESH
SP = ("outer", "pair")
AXES = ("outer", "pair", "tp")
LANES = 128
PAD = 16
ROWS = 64
F32, BF16 = jnp.float32, jnp.bfloat16


def sigmoid(value):
    return 1.0 / (1.0 + jnp.exp(-value))


def dot(left, right):
    return jnp.dot(left, right, preferred_element_type=F32)


class Sends:
    def __init__(self, sems):
        self.sems, self.open = sems, []

    def start(self, src, dst, recv, device):
        copy = pltpu.make_async_remote_copy(
            src_ref=src, dst_ref=dst, send_sem=self.sems.at[len(self.open)],
            recv_sem=recv, device_id=device, device_id_type=MESH,
        )
        copy.start()
        self.open.append((copy, None))

    def start_if(self, cond, src, dst, recv, device):
        copy = pltpu.make_async_remote_copy(
            src_ref=src, dst_ref=dst, send_sem=self.sems.at[len(self.open)],
            recv_sem=recv, device_id=device, device_id_type=MESH,
        )
        pl.when(cond)(copy.start)
        self.open.append((copy, cond))

    def drain(self):
        for copy, cond in self.open:
            if cond is None:
                copy.wait_send()
            else:
                pl.when(cond)(copy.wait_send)


def arrived(ref, recv):
    pltpu.make_async_copy(ref, ref, recv).wait()


JOBS = 3


def dot_tokens(left, right):
    return lax.dot_general(left, right, (((0,), (0,)), ((), ())), preferred_element_type=F32)


def dot_channels(left, right):
    return lax.dot_general(left, right, (((1,), (1,)), ((), ())), preferred_element_type=F32)


def loop(count, body):
    def step(index, carry):
        body(index)
        return carry

    lax.fori_loop(0, count, step, 0)


def kernel(
    n, n_tp, conv,
    x_ref, g_ref, wv_ref, wg_ref, wo_ref, taps_in, gain_ref,
    gi_out, gvw_out, ggw_out, gow_out, taps_out, gain_out, px_in, line_in, gi_in,
    taps_ref, both, weights, pool, hp, gc, ag, rs, own_right, pair_right, pair_left, line, gi_sent, gi_own, gi_total, xs, xr,
    sum_a, sum_b, mean_b, inv_b, stat1, stat2, small, small_x, group, group_in, group_all, taps_total, gain_total,
    send_sems, recv_x, recv_g, recv_px, recv_line, recv_h, recv_c, recv_s1, recv_s2, own_sems, weight_sems,
    left_sems, line_sems, out_sems,
    ag_send, ag_recv, rs_send, rs_recv, xr_send, xr_recv, swap_send, swap_recv, gi_send, gi_recv,
    sx_send, sx_recv, s1_send, s1_recv, s2_send, s2_recv,
):
    z, pair, tp = (lax.axis_index(name) for name in AXES)
    last, mirror = n - 1, n - 1 - z
    seq, n_seq, per = z * 2 + pair, n * 2, (n * 2) // n_tp
    tokens, width, half = both.shape[2], both.shape[3], own_right.shape[2]
    n_lane, total = hp.shape[0], width * n_seq
    n_half = n_lane // 2
    sibling, core, n_y = tp + 1 - 2 * lax.rem(tp, 2), lax.rem(tp, 2), n_tp // 2
    across = [lax.rem(tp + 2 * step, n_tp) for step in range(1, n_y)]
    radius = conv // 2
    before, after = seq - 1, seq + 1
    has_before, has_after = seq > 0, seq < n_seq - 1
    home = lambda index: (z, pair, index)
    beside = lambda index: (lax.div(index, 2), lax.rem(index, 2), tp)
    level = lambda index: (index, pair, tp)
    facing = (z, 1 - pair, tp)
    planes = [lax.rem(z + step, n) for step in range(1, n)]
    gg, xg = both.at[0], both.at[1]
    PV, PS, GA, CV = 0, n_lane, 2 * n_lane, 3 * n_lane

    barrier = pltpu.get_barrier_semaphore()

    def greet(device):
        pl.semaphore_signal(barrier, inc=1, device_id=device, device_id_type=MESH)

    for step in range(1, n_tp):
        greet(home(lax.rem(tp + step, n_tp)))
    pl.when(has_before)(lambda: greet(beside(before)))
    pl.when(has_after)(lambda: greet(beside(after)))
    greet(facing)
    for other in planes:
        greet(level(other))

    def load(src, dst, sem):
        copy = pltpu.make_async_copy(src, dst, sem)
        copy.start()
        return copy

    def remote(src, dst, send, recv, device):
        return pltpu.make_async_remote_copy(
            src_ref=src, dst_ref=dst, send_sem=send, recv_sem=recv, device_id=device, device_id_type=MESH
        )

    block = lambda b, h: b * per + h
    order = [tp, sibling]
    for other in across:
        order += [other, other + 1 - 2 * core]

    places = [(False, r) for r in range(2 * per)] + [(True, r) for r in range(2 * per)]
    for wanted in (False, True):
        for step in range(n_y - 1):
            for h in range(per):
                places += [(wanted, (2 + 2 * step) * per + h), (wanted, (3 + 2 * step) * per + h)]

    def streams(turn):
        wanted, rank = places[turn]
        index = block(order[rank // per], rank % per)
        row = pl.multiple_of(index * width, width)
        return index, [
            pltpu.make_async_copy(ref.at[pl.ds(row, width), :], weights.at[turn % 2, i], weight_sems.at[turn % 2, i])
            for i, ref in enumerate((wo_ref,) if wanted else (wv_ref, wg_ref))
        ]

    for c in range(n_lane):
        taps_ref[c, 0:conv, :] = taps_in[:, c * LANES : (c + 1) * LANES].astype(F32)

    def gain_of(c):
        return gain_ref[:, pl.ds(pl.multiple_of(c * LANES, LANES), LANES)]

    owns = []
    for name, (hbm, vmem) in enumerate(((x_ref, xg), (g_ref, gg))):
        owns.append([
            load(hbm.at[:, pl.ds(h * width, width)], vmem.at[block(tp, h)], own_sems.at[name, h]) for h in range(per)
        ])
    for copy in streams(0)[1]:
        copy.start()

    count = n_tp - 1 + 1 + n - 1 + has_before.astype(jnp.int32) + has_after.astype(jnp.int32)
    pl.semaphore_wait(barrier, count)

    sends = Sends(send_sems)
    for hbm, vmem, recv in ((x_ref, xg, recv_x), (g_ref, gg, recv_g)):
        for h in range(per):
            src, index = hbm.at[:, pl.ds(h * width, width)], block(tp, h)
            for other in [sibling] + across:
                sends.start(src, vmem.at[index], recv.at[index], home(other))
    crossing = pl.multiple_of((1 - pair) * width, width)
    sends.start(x_ref.at[:, pl.ds(crossing, width)], px_in.at[tp], recv_px.at[tp], facing)

    part, n_part = lax.div(tp, 2), tokens // n_y

    def part_rows(index):
        start = index * n_part
        return pl.ds(start if isinstance(index, int) else pl.multiple_of(start, n_part), n_part)


    def line_send(tensor, src, b, cond):
        sends.start_if(
            jnp.logical_and(cond, b != z), src, line_in.at[tensor, z, core, part_rows(part)],
            recv_line.at[tensor, z, core, part], level(b),
        )

    column = pl.multiple_of(core * width, width)
    line_send(1, x_ref.at[part_rows(part), pl.ds(column, width)], tp, True)

    turns = iter(range(len(places)))

    def project(left):
        turn = next(turns)
        wanted, rank = places[turn]
        index, copies = streams(turn)
        if turn + 1 < len(places):
            for copy in streams(turn + 1)[1]:
                copy.start()
        for copy in copies:
            copy.wait()

        def body(j):
            cols = pl.ds(pl.multiple_of(j * 256, 256), 256)
            for i, base in enumerate((GA,) if wanted else (PV, PS)):
                value = dot(left[index], weights[turn % 2, i, :, cols])
                for side in range(2):
                    piece = value[:, side * LANES : (side + 1) * LANES]
                    if rank == 0:
                        pool[base + 2 * j + side] = piece
                    else:
                        pool[base + 2 * j + side] += piece

        loop(n_lane // 2, body)

    def land(vmem, recv, b, h):
        index = block(b, h)
        arrived(vmem.at[index], recv.at[index])
        sends.start(vmem.at[index], vmem.at[index], recv.at[index], home(sibling))

    def near(tensor, vmem, recv):
        for copy in owns[1 - tensor]:
            copy.wait()
        for h in range(per):
            project(vmem)
        for h in range(per):
            index = block(sibling, h)
            arrived(vmem.at[index], recv.at[index])
        if tensor == 1:
            line_send(1, xg.at[block(sibling, core), part_rows(part)], sibling, True)
        for h in range(per):
            project(vmem)

    def far(tensor, vmem, recv, between):
        for other in across:
            for h in range(per):
                if other is across[-1] and h == per - 1:
                    between()
                land(vmem, recv, other, h)
                line_send(tensor, vmem.at[block(other, h), part_rows(part)], other, core == h)
                if tensor == 1:
                    sends.start_if(h != pair, vmem.at[block(other, h)], px_in.at[other], recv_px.at[other], facing)
                project(vmem)
                index = block(other + 1 - 2 * core, h)
                arrived(vmem.at[index], recv.at[index])
                line_send(tensor, vmem.at[index, part_rows(part)], other + 1 - 2 * core, core == h)
                project(vmem)

    near(1, xg, recv_x)
    near(0, gg, recv_g)
    far(1, xg, recv_x, lambda: None)

    def gate(i):
        c, r = lax.div(i, tokens // ROWS), lax.rem(i, tokens // ROWS)
        rows = pl.ds(pl.multiple_of(r * ROWS, ROWS), ROWS)
        sig = sigmoid(pool[PS + c, rows, :])
        pool[PS + c, rows, :] = sig
        hp[c, pl.ds(pl.multiple_of(r * ROWS + PAD, 8), ROWS), :] = (pool[PV + c, rows, :] * sig).astype(BF16).astype(F32)

    loop(n_lane * (tokens // ROWS), gate)

    def halo(buffer, recv):
        @pl.when(jnp.logical_not(has_before))
        def _():
            buffer[:, 0:PAD, :] = jnp.zeros((n_lane, PAD, LANES), F32)

        @pl.when(jnp.logical_not(has_after))
        def _():
            buffer[:, PAD + tokens : 2 * PAD + tokens, :] = jnp.zeros((n_lane, PAD, LANES), F32)

        sends.start_if(has_after, buffer.at[:, pl.ds(tokens, PAD), :], buffer.at[:, pl.ds(0, PAD), :], recv.at[0], beside(after))
        sends.start_if(has_before, buffer.at[:, pl.ds(PAD, PAD), :], buffer.at[:, pl.ds(PAD + tokens, PAD), :], recv.at[1], beside(before))

    def halo_here(buffer, recv):
        pl.when(has_before)(lambda: arrived(buffer.at[:, pl.ds(0, PAD), :], recv.at[0]))
        pl.when(has_after)(lambda: arrived(buffer.at[:, pl.ds(PAD + tokens, PAD), :], recv.at[1]))

    halo(hp, recv_h)
    line_send(0, g_ref.at[part_rows(part), pl.ds(column, width)], tp, True)
    line_send(0, gg.at[block(sibling, core), part_rows(part)], sibling, True)

    def convolve(r):
        rows = pl.ds(pl.multiple_of(r * ROWS, ROWS), ROWS)

        def lane(c, carry):
            first, second = carry
            value = jnp.zeros((ROWS, LANES), F32)
            for k in range(conv):
                value = value + taps_ref[c, k : k + 1, :] * hp[c, pl.ds(r * ROWS + (PAD + k - radius), ROWS), :]
            pool[CV + c, rows, :] = value
            return first + value, second + value * value

        zero = jnp.zeros((ROWS, LANES), F32)
        first, second = lax.fori_loop(0, n_lane, lane, (zero, zero))
        sum_a[rows, :] = first
        sum_b[rows, :] = second

    def inner_rows(body):
        def step(r, carry):
            body(r)
            return carry

        lax.fori_loop(1, tokens // ROWS - 1, step, 0)

    inner_rows(convolve)
    halo_here(hp, recv_h)
    convolve(0)
    convolve(tokens // ROWS - 1)

    def to_row(value):
        return jnp.sum(value.T, axis=0, keepdims=True)

    def to_rows(row):
        return jnp.broadcast_to(row, (LANES, tokens)).T

    def send_sums(stat, recv):
        stat[tp, 0:1, :] = to_row(sum_a[...])
        stat[tp, 1:2, :] = to_row(sum_b[...])
        for step in range(1, n_tp):
            sends.start(stat.at[tp], stat.at[tp], recv.at[tp], home(lax.rem(tp + step, n_tp)))

    def take_sums(stat, recv):
        for step in range(1, n_tp):
            other = lax.rem(tp + step, n_tp)
            arrived(stat.at[other], recv.at[other])
        first, second = stat[0, 0:1, :], stat[0, 1:2, :]
        for other in range(1, n_tp):
            first, second = first + stat[other, 0:1, :], second + stat[other, 1:2, :]
        return first / total, second / total

    send_sums(stat1, recv_s1)

    lane_of = lambda c: pl.ds(pl.multiple_of(lax.rem(c, n_half) * LANES, LANES), LANES)

    def ag_right(k, j):
        return remote(ag.at[j, z - k], ag.at[j, z - k], ag_send.at[0, j, k], ag_recv.at[j, z - k], level(z + 1))

    def ag_left(k, j):
        return remote(ag.at[j, z + k], ag.at[j, z + k], ag_send.at[1, j, k], ag_recv.at[j, z + k], level(z - 1))

    def leave(j):
        pl.when(z < last)(lambda: ag_right(0, j).start())
        pl.when(z > 0)(lambda: ag_left(0, j).start())

    def activate():
        mean, square = take_sums(stat1, recv_s1)
        mean_b[...] = to_rows(mean)
        inv_b[...] = to_rows(lax.rsqrt(square - mean * mean + 1e-06))
        small[:, conv : conv + 1, :] = jnp.zeros((n_lane, 1, LANES), F32)

        def step(r):
            rows = pl.ds(pl.multiple_of(r * ROWS, ROWS), ROWS)
            mean_r, inv_r = mean_b[rows, :], inv_b[rows, :]

            def lane(c):
                normed = (pool[CV + c, rows, :] - mean_r) * inv_r
                pool[CV + c, rows, :] = normed
                scaled = normed * gain_of(c)
                ag[lax.div(c, n_half), z, rows, lane_of(c)] = (scaled * sigmoid(scaled)).astype(BF16)

            loop(n_lane, lane)

        loop(tokens // ROWS, step)

    far(0, gg, recv_g, activate)
    def backward(r, carry):
        rows = pl.ds(pl.multiple_of(r * ROWS, ROWS), ROWS)

        def lane(c, carry):
            first, second = carry
            normed = pool[CV + c, rows, :]
            gain = gain_of(c)
            scaled = normed * gain
            sig = sigmoid(scaled)
            grad_scaled = pool[GA + c, rows, :] * sig * (1.0 + scaled * (1.0 - sig))
            small[c, conv : conv + 1, :] += jnp.sum(grad_scaled * normed, axis=0, keepdims=True)
            grad_normed = grad_scaled * gain
            gc[c, pl.ds(pl.multiple_of(r * ROWS + PAD, 8), ROWS), :] = grad_normed
            return first + grad_normed, second + grad_normed * normed

        zero = jnp.zeros((ROWS, LANES), F32)
        first, second = lax.fori_loop(0, n_lane, lane, (zero, zero))
        sum_a[rows, :] = first
        sum_b[rows, :] = second
        return carry

    lax.fori_loop(0, tokens // ROWS, backward, 0)
    send_sums(stat2, recv_s2)

    def line_here(tensor, source, h, piece):
        ref = line_in.at[tensor, source, h, part_rows(piece)]
        arrived(ref, recv_line.at[tensor, source, h, piece])
        return ref

    def line_share(tensor):
        for source in planes:
            ref = line_here(tensor, source, core, part)
            for other in across + [sibling]:
                sends.start(ref, ref, recv_line.at[tensor, source, core, part], home(other))

    def line_pass(tensor):
        for source in planes:
            for step in range(1, n_y):
                piece = lax.rem(part + step, n_y)
                ref = line_here(tensor, source, core, piece)
                sends.start(ref, ref, recv_line.at[tensor, source, core, piece], home(sibling))

    def line_end(tensor):
        for source in planes:
            for piece in range(n_y):
                line_here(tensor, source, 1 - core, piece)

    line_share(1)
    mine = [tp] + across
    for b in mine:
        arrived(px_in.at[b], recv_px.at[b])
        sends.start(px_in.at[b], px_in.at[b], recv_px.at[b], home(sibling))
    first_mean, second_mean = take_sums(stat2, recv_s2)
    sum_a[...] = to_rows(first_mean)
    sum_b[...] = to_rows(second_mean)

    def finish(r):
        rows = pl.ds(pl.multiple_of(r * ROWS, ROWS), ROWS)
        padded = pl.ds(pl.multiple_of(r * ROWS + PAD, 8), ROWS)
        inv_r, first_r, second_r = inv_b[rows, :], sum_a[rows, :], sum_b[rows, :]

        def lane(c, carry):
            gc[c, padded, :] = inv_r * (gc[c, padded, :] - first_r - pool[CV + c, rows, :] * second_r)
            return carry

        lax.fori_loop(0, n_lane, lane, 0)

    finish(0)
    finish(tokens // ROWS - 1)
    halo(gc, recv_c)
    leave(0)
    leave(1)
    inner_rows(finish)

    def spread(r):
        rows = pl.ds(pl.multiple_of(r * ROWS, ROWS), ROWS)

        def lane(c, carry):
            value = jnp.zeros((ROWS, LANES), F32)
            for k in range(conv):
                value = value + taps_ref[c, k : k + 1, :] * gc[c, pl.ds(r * ROWS + (PAD + radius - k), ROWS), :]
            sig = pool[PS + c, rows, :]
            own_right[lax.div(c, n_half), rows, lane_of(c)] = (value * sig).astype(BF16)
            grad_gate = (value * pool[PV + c, rows, :] * sig * (1.0 - sig)).astype(BF16)

            @pl.when(c < n_half)
            def _():
                own_right[2, rows, lane_of(c)] = grad_gate

            @pl.when(c >= n_half)
            def _():
                ag[2, z, rows, lane_of(c)] = grad_gate

            return carry

        lax.fori_loop(0, n_lane, lane, 0)

    inner_rows(spread)
    halo_here(gc, recv_c)
    spread(0)
    spread(tokens // ROWS - 1)

    steps = n_tp * per

    def weight_copies(s, slot):
        b, h = lax.rem(tp + 1 + lax.div(s, per), n_tp), lax.rem(s, per)
        row = pl.multiple_of((b * per + h) * width, width)
        return [
            pltpu.make_async_copy(ref.at[pl.ds(row, width), :], weights.at[slot, i], weight_sems.at[slot, i])
            for i, ref in enumerate((wv_ref, wg_ref))
        ]

    for copy in weight_copies(0, 0):
        copy.start()
    for b in mine:
        twin = b + 1 - 2 * core
        arrived(px_in.at[twin], recv_px.at[twin])
    lefts = [load(px_in.at[d], pair_left.at[d], left_sems.at[d]) for d in range(n)]
    leave(2)
    swaps = [remote(own_right.at[j], pair_right.at[j], swap_send.at[j], swap_recv.at[j], facing) for j in range(JOBS)]
    for copy in swaps:
        copy.start()
    line_share(0)

    lead, trail = pl.ds(0, half), pl.ds(half, half)

    def input_step(s):
        slot = lax.rem(s, 2)

        @pl.when(s < steps - 1)
        def _():
            for copy in weight_copies(s + 1, 1 - slot):
                copy.start()

        for copy in weight_copies(s, slot):
            copy.wait()
        b, h = lax.rem(tp + 1 + lax.div(s, per), n_tp), lax.rem(s, per)
        value = dot_channels(own_right[0], weights[slot, 0, :, lead]) + dot_channels(own_right[1], weights[slot, 0, :, trail])
        value = value + dot_channels(own_right[2], weights[slot, 1, :, lead])
        value = (value + dot_channels(ag[2, z], weights[slot, 1, :, trail])).astype(BF16)

        @pl.when(s < steps - per)
        def _():
            gi_sent[s] = value
            remote(gi_sent.at[s], gi_in.at[tp, h], gi_send.at[s], gi_recv.at[tp, h], home(b)).start()

        @pl.when(s >= steps - per)
        def _():
            gi_own[h] = value

    loop(steps // 2, input_step)
    line_pass(1)
    for copy in lefts:
        copy.wait()
    rows = group.shape[2]

    def tap_sums(c):
        def step(r, sums):
            row = pl.multiple_of(r * 8, 8)
            grad = gc[c, pl.ds(pl.multiple_of(row + PAD, 8), 8), :]
            return tuple(sums[k] + hp[c, pl.ds(row + (PAD + k - radius), 8), :] * grad for k in range(conv))

        zeros = tuple(jnp.zeros((8, LANES), F32) for _ in range(conv))
        sums = lax.fori_loop(0, (hp.shape[1] - 2 * PAD) // 8, step, zeros)
        for k in range(conv):
            small[c, k : k + 1, :] = jnp.sum(sums[k], axis=0, keepdims=True)

    def keep(kind, j, value, add):
        for i in range(n_half):
            index, piece = (kind * JOBS + j) * n_half + i, value[:, i * LANES : (i + 1) * LANES]
            if add:
                pool[index, 0:width, :] += piece
            else:
                pool[index, 0:width, :] = piece

    def partial_rows(j, d):
        return dot_tokens(both[1, d * 2 + pair], own_right[j]) + dot_tokens(pair_left[d], pair_right[j])

    def own_rows(j):
        keep(0, j, partial_rows(j, z), False)
        tensor, cells = lax.div(j, 2), ag[j, z]
        keep(1, j, dot_tokens(both[tensor, z * 2 + pair], cells), False)
        keep(2, j, dot_tokens(both[tensor, z * 2 + 1 - pair], cells), False)

    def line_rows(j, source, side):
        tensor, cells = lax.div(j, 2), ag[j, source]
        keep(1, j, dot_tokens(line[side, tensor, pair], cells), True)
        keep(2, j, dot_tokens(line[side, tensor, 1 - pair], cells), True)

    def line_load(k, action):
        for side, (cond, source) in enumerate(((k <= z, z - k), (k <= mirror, z + k))):
            @pl.when(cond)
            def _():
                for tensor in range(2):
                    action(pltpu.make_async_copy(line_in.at[tensor, source], line.at[side, tensor], line_sems.at[side, tensor]))

    def rs_right(j, d):
        return remote(rs.at[j, d], rs.at[j, d], rs_send.at[j, d], rs_recv.at[j, d], level(z + 1))

    def rs_left(j, d):
        slot = jnp.where(d == z - 1, n, d)
        return remote(rs.at[j, d], rs.at[j, slot], rs_send.at[j, d], rs_recv.at[j, slot], level(z - 1))

    def reduce_step(j, d, waiting, copy):
        value = partial_rows(j, d)

        @pl.when(waiting)
        def _():
            arrived(rs.at[j, d], rs_recv.at[j, d])
            rs[j, d] = (value + rs[j, d].astype(F32)).astype(BF16)

        @pl.when(jnp.logical_not(waiting))
        def _():
            rs[j, d] = value.astype(BF16)

        copy(j, d).start()

    farthest = jnp.maximum(z, mirror)
    small_swap = remote(small, small_x, sx_send.at[0], sx_recv.at[0], facing)

    def add_lines(j, k):
        pl.when(k <= z)(lambda: line_rows(j, z - k, 0))
        pl.when(k <= mirror)(lambda: line_rows(j, z + k, 1))

        @pl.when(k == farthest)
        def _():
            for i in range(n_half):
                xs[j, :, i * LANES : (i + 1) * LANES] = pool[(2 * JOBS + j) * n_half + i, 0:width, :].astype(BF16)
            remote(xs.at[j], xr.at[j], xr_send.at[j], xr_recv.at[j], facing).start()

    def period(k, first):
        if not first:
            line_load(k, lambda copy: copy.start())

        def job(j):
            @pl.when(k <= z)
            def _():
                arrived(ag.at[j, z - k], ag_recv.at[j, z - k])
                pl.when(z < last)(lambda: ag_right(k, j).start())

            @pl.when(k <= mirror)
            def _():
                arrived(ag.at[j, z + k], ag_recv.at[j, z + k])
                pl.when(z > 0)(lambda: ag_left(k, j).start())

            if first:
                arrived(pair_right.at[j], swap_recv.at[j])

            @pl.when(jnp.logical_and(z < last, k > z))
            def _():
                reduce_step(j, n + z - k, z > 0, rs_right)

            @pl.when(jnp.logical_and(z > 0, k > mirror))
            def _():
                reduce_step(j, k - mirror - 1, z < last, rs_left)

            if not first:
                pl.when(j == 0)(lambda: line_load(k, lambda copy: copy.wait()))
                add_lines(j, k)

        loop(JOBS, job)

    period(1, True)
    loop(steps - steps // 2, lambda s: input_step(s + steps // 2))
    line_pass(0)
    loop(n_lane, tap_sums)
    line_end(1)
    line_end(0)
    line_load(1, lambda copy: copy.start())
    small_swap.start()
    loop(JOBS, own_rows)
    small_swap.wait_recv()
    for g in range(n):
        group[g] = small[:, g * rows : (g + 1) * rows, :] + small_x[:, g * rows : (g + 1) * rows, :]
    group_in[z] = group[z]
    for step in range(1, n):
        other = lax.rem(z + step, n)
        remote(group.at[other], group_in.at[z], s1_send.at[step], s1_recv.at[z], level(other)).start()
    line_load(1, lambda copy: copy.wait())
    loop(JOBS, lambda j: add_lines(j, 1))

    def share_sums():
        for step in range(1, n):
            other = lax.rem(z + step, n)
            arrived(group_in.at[other], s1_recv.at[other])
        value = group_in[0]
        for other in range(1, n):
            value = value + group_in[other]
        group_all[z] = value
        for step in range(1, n):
            remote(group_all.at[z], group_all.at[z], s2_send.at[step], s2_recv.at[z], level(lax.rem(z + step, n))).start()

    def later(index):
        pl.when(index == 1)(share_sums)
        period(index + 2, False)

    loop(last - 1, later)

    loop(steps - per, lambda s: remote(gi_sent.at[s], gi_in.at[tp, 0], gi_send.at[s], gi_recv.at[tp, 0], facing).wait_send())
    arrivals = []
    for step in range(1, n_tp):
        other = lax.rem(tp + step, n_tp)
        for h in range(per):
            arrived(gi_in.at[other, h], gi_recv.at[other, h])
            slot = (step - 1) * per + h
            arrivals.append(load(gi_in.at[other, h], gi_sent.at[slot], gi_send.at[slot]))
    for copy in arrivals:
        copy.wait()
    for h in range(per):
        value = gi_own[h].astype(F32)
        for step in range(1, n_tp):
            value = value + gi_sent[(step - 1) * per + h].astype(F32)
        gi_total[:, h * width : (h + 1) * width] = value.astype(BF16)
    outs = [load(gi_total, gi_out, out_sems.at[0])]
    for step in range(1, n):
        other = lax.rem(z + step, n)
        arrived(group_all.at[other], s2_recv.at[other])
    for g in range(n):
        kept = min(rows, conv - g * rows)
        for c in range(n_lane):
            columns = slice(c * LANES, (c + 1) * LANES)
            taps_total[g * rows : g * rows + kept, columns] = group_all[g, c, :kept]
            if kept < rows:
                gain_total[:, columns] = group_all[g, c, kept:]
    outs.append(load(taps_total, taps_out, out_sems.at[1]))
    outs.append(load(gain_total, gain_out, out_sems.at[8]))

    def settle(kind, j, slot, into):
        for i in range(n_half):
            cols = slice(i * LANES, (i + 1) * LANES)
            value = pool[(kind * JOBS + j) * n_half + i, 0:width, :]
            for ref in slot:
                value = value + ref[:, cols].astype(F32)
            into[:, cols] = value.astype(BF16)

    for j, (ref, columns) in enumerate(((gow_out, lead), (gow_out, trail), (ggw_out, trail))):
        arrived(xr.at[j], xr_recv.at[j])
        settle(1, j, (xr.at[j],), xr.at[j])
        outs.append(load(xr.at[j], ref.at[:, columns], out_sems.at[2 + j]))
    for j, (ref, columns) in enumerate(((gvw_out, lead), (gvw_out, trail), (ggw_out, lead))):
        lower, upper = rs.at[j, z], rs.at[j, n]
        pl.when(z > 0)(lambda: arrived(lower, rs_recv.at[j, z]))
        pl.when(z < last)(lambda: arrived(upper, rs_recv.at[j, n]))
        pl.when(z == 0)(lambda: settle(0, j, (upper,), lower))
        pl.when(z == last)(lambda: settle(0, j, (lower,), lower))
        pl.when(jnp.logical_and(z > 0, z < last))(lambda: settle(0, j, (lower, upper), lower))
        outs.append(load(lower, ref.at[:, columns], out_sems.at[5 + j]))

    def sent(j):
        def step(k):
            pl.when(jnp.logical_and(k <= z, z < last))(lambda: ag_right(k, j).wait_send())
            pl.when(jnp.logical_and(k <= mirror, z > 0))(lambda: ag_left(k, j).wait_send())
            pl.when(k > z)(lambda: rs_right(j, k).wait_send())
            pl.when(k < z)(lambda: rs_left(j, k).wait_send())

        loop(n, step)
        remote(xs.at[j], xr.at[j], xr_send.at[j], xr_recv.at[j], facing).wait_send()

    loop(JOBS, sent)
    for copy in swaps + [small_swap]:
        copy.wait_send()
    sends.drain()
    for step in range(1, n):
        remote(group.at[0], group_in.at[z], s1_send.at[step], s1_recv.at[z], facing).wait_send()
        remote(group_all.at[z], group_all.at[z], s2_send.at[step], s2_recv.at[z], facing).wait_send()
    for copy in outs:
        copy.wait()


def local(inputs, w_value, w_gate, taps, ln_gain, w_out, grad_out):
    n, n_tp = lax.axis_size("outer"), lax.axis_size("tp")
    n_seq = n * 2
    tokens, own = inputs.shape
    conv, channels = taps.shape
    width = own * n_tp // n_seq
    per, n_lane, n_y, half = n_seq // n_tp, channels // LANES, n_tp // 2, channels // 2
    n_sends = (
        2 * per * n_y + 1 + 2 + 2 + 2 * 3 * (n_y - 1) * per + (n_y - 1) * per + 4 + 2 * (n_tp - 1)
        + 2 * (n - 1) * (2 * n_y - 1) + n_y
    )
    any_spec, vmem_spec = pl.BlockSpec(memory_space=pl.ANY), pl.BlockSpec(memory_space=pltpu.VMEM)
    dma = lambda *shape: pltpu.SemaphoreType.DMA(shape)
    bf, wide = (lambda *shape: pltpu.VMEM(shape, BF16)), (lambda *shape: pltpu.VMEM(shape, F32))
    out_shapes = [
        ((tokens, own), BF16), *[((width, channels), BF16)] * 3, ((conv, channels), F32), ((1, channels), F32),
        ((n_tp, tokens, width), BF16), ((2, n, 2, tokens, width), BF16), ((n_tp, per, tokens, width), BF16),
    ]
    n_gi, rows = (n_tp - 1) * per, (conv + 1) // n
    results = pl.pallas_call(
        functools.partial(kernel, n, n_tp, conv),
        name="module_backward",
        out_shape=[jax.ShapeDtypeStruct(shape, dtype) for shape, dtype in out_shapes],
        in_specs=[any_spec] * 5 + [vmem_spec] * 2,
        out_specs=[any_spec] * len(out_shapes),
        scratch_shapes=[
            wide(n_lane, conv + 1, LANES), bf(2, n_seq, tokens, width), bf(2, 2, width, channels), wide(4 * n_lane + n_lane // 2, tokens, LANES),
            wide(n_lane, tokens + 2 * PAD, LANES), wide(n_lane, tokens + 2 * PAD, LANES),
            bf(JOBS, n, tokens, half), bf(JOBS, n + 1, width, half), bf(JOBS, tokens, half), bf(JOBS, tokens, half),
            bf(n, tokens, width), bf(2, 2, 2, tokens, width),
            bf(n_gi, tokens, width), bf(per, tokens, width), bf(tokens, own),
            bf(JOBS, width, half), bf(JOBS, width, half),
            *[wide(tokens, LANES)] * 4, *[wide(n_tp, 8, tokens)] * 2,
            wide(n_lane, conv + 1, LANES), wide(n_lane, conv + 1, LANES),
            *[wide(n, n_lane, rows, LANES)] * 3, wide(conv, channels), wide(1, channels),
            dma(n_sends), dma(n_seq), dma(n_seq), dma(n_tp), dma(2, n, 2, n_y), dma(2), dma(2), dma(n_tp), dma(n_tp),
            dma(2, per), dma(2, 2), dma(n), dma(2, 2), dma(9),
            dma(2, JOBS, n), dma(JOBS, n), dma(JOBS, n + 1), dma(JOBS, n + 1), dma(JOBS), dma(JOBS), dma(JOBS), dma(JOBS),
            dma(n_gi), dma(n_tp, per),
            dma(1), dma(1), dma(n), dma(n), dma(n), dma(n),
        ],
        compiler_params=pltpu.CompilerParams(
            collective_id=0, has_side_effects=True, vmem_limit_bytes=67043328
        ),
        cost_estimate=pl.CostEstimate(
            flops=2 * 8 * tokens * width * n_seq * channels, bytes_accessed=80 * 2**20, transcendentals=0
        ),
    )(inputs, grad_out, w_value, w_gate, w_out, taps, ln_gain.reshape(1, channels))
    parts = 4
    block = lambda shape: pl.BlockSpec((shape[0] // parts, shape[1]), lambda i: (i, 0))
    fixed = lambda shape: pl.BlockSpec(shape, lambda i: (0, 0))
    shapes = [shape for shape, dtype in out_shapes[:6]]
    specs = [block(shape) for shape in shapes[:4]] + [fixed(shape) for shape in shapes[4:]]

    def write(*refs):
        for source, target in zip(refs[:6], refs[6:]):
            target[...] = source[...].astype(target.dtype)

    written = pl.pallas_call(
        write,
        name="write_results",
        grid=(parts,),
        out_shape=[jax.ShapeDtypeStruct(shape, F32 if i else BF16) for i, shape in enumerate(shapes)],
        in_specs=specs,
        out_specs=specs,
        cost_estimate=pl.CostEstimate(flops=0, bytes_accessed=11 * 2**20, transcendentals=0),
    )(*results[:6])
    return (*written[:5], written[5][0])


def solution(mesh):
    count, across = mesh.devices.shape
    fine = Mesh(mesh.devices.reshape(count // 2, 2, across), AXES)
    in_specs = (P(SP, "tp"), P(None, "tp"), P(None, "tp"), P(None, "tp"), P("tp"), P(None, "tp"), P(SP, "tp"))
    out_specs = (P(SP, "tp"), P(SP, "tp"), P(SP, "tp"), P(SP, "tp"), P(None, "tp"), P("tp"))
    return jax.shard_map(local, mesh=fine, in_specs=in_specs, out_specs=out_specs, check_vma=False)
```

```python
import functools

import jax
import jax.numpy as jnp
from jax import lax
from jax.experimental import pallas as pl
from jax.experimental.pallas import tpu as pltpu
from jax.sharding import Mesh, PartitionSpec as P

MESH = pl.DeviceIdType.MESH
SP = ("outer", "pair")
AXES = ("outer", "pair", "tp")
LANES = 128
PAD = 16
ROWS = 64
F32, BF16 = jnp.float32, jnp.bfloat16


def sigmoid(value):
    return 1.0 / (1.0 + jnp.exp(-value))


def dot(left, right):
    return jnp.dot(left, right, preferred_element_type=F32)


class Sends:
    def __init__(self, sems):
        self.sems, self.open = sems, []

    def start(self, src, dst, recv, device):
        copy = pltpu.make_async_remote_copy(
            src_ref=src, dst_ref=dst, send_sem=self.sems.at[len(self.open)],
            recv_sem=recv, device_id=device, device_id_type=MESH,
        )
        copy.start()
        self.open.append((copy, None))

    def start_if(self, cond, src, dst, recv, device):
        copy = pltpu.make_async_remote_copy(
            src_ref=src, dst_ref=dst, send_sem=self.sems.at[len(self.open)],
            recv_sem=recv, device_id=device, device_id_type=MESH,
        )
        pl.when(cond)(copy.start)
        self.open.append((copy, cond))

    def drain(self):
        for copy, cond in self.open:
            if cond is None:
                copy.wait_send()
            else:
                pl.when(cond)(copy.wait_send)


def arrived(ref, recv):
    pltpu.make_async_copy(ref, ref, recv).wait()


JOBS = 3


def dot_tokens(left, right):
    return lax.dot_general(left, right, (((0,), (0,)), ((), ())), preferred_element_type=F32)


def dot_channels(left, right):
    return lax.dot_general(left, right, (((1,), (1,)), ((), ())), preferred_element_type=F32)


def loop(count, body):
    def step(index, carry):
        body(index)
        return carry

    lax.fori_loop(0, count, step, 0)


def kernel(
    n, n_tp, conv,
    x_ref, g_ref, wv_ref, wg_ref, wo_ref, taps_in, gain_ref,
    gi_out, gvw_out, ggw_out, gow_out, taps_out, gain_out, px_in, line_in, gi_in,
    taps_ref, both, weights, pool, hp, gc, ag, rs, own_right, pair_right, pair_left, line, gi_sent, gi_own, gi_total, xs, xr,
    sum_a, sum_b, mean_b, inv_b, stat1, stat2, small, small_x, group, group_in, group_all, taps_total, gain_total,
    send_sems, recv_x, recv_g, recv_px, recv_line, recv_h, recv_c, recv_s1, recv_s2, own_sems, weight_sems,
    left_sems, line_sems, out_sems,
    ag_send, ag_recv, rs_send, rs_recv, xr_send, xr_recv, swap_send, swap_recv, gi_send, gi_recv,
    sx_send, sx_recv, s1_send, s1_recv, s2_send, s2_recv,
):
    z, pair, tp = (lax.axis_index(name) for name in AXES)
    last, mirror = n - 1, n - 1 - z
    seq, n_seq, per = z * 2 + pair, n * 2, (n * 2) // n_tp
    tokens, width, half = both.shape[2], both.shape[3], own_right.shape[2]
    n_lane, total = hp.shape[0], width * n_seq
    n_half = n_lane // 2
    sibling, core, n_y = tp + 1 - 2 * lax.rem(tp, 2), lax.rem(tp, 2), n_tp // 2
    across = [lax.rem(tp + 2 * step, n_tp) for step in range(1, n_y)]
    radius = conv // 2
    before, after = seq - 1, seq + 1
    has_before, has_after = seq > 0, seq < n_seq - 1
    home = lambda index: (z, pair, index)
    beside = lambda index: (lax.div(index, 2), lax.rem(index, 2), tp)
    level = lambda index: (index, pair, tp)
    facing = (z, 1 - pair, tp)
    planes = [lax.rem(z + step, n) for step in range(1, n)]
    gg, xg = both.at[0], both.at[1]
    PV, PS, GA, CV = 0, n_lane, 2 * n_lane, 3 * n_lane

    barrier = pltpu.get_barrier_semaphore()

    def greet(device):
        pl.semaphore_signal(barrier, inc=1, device_id=device, device_id_type=MESH)

    for step in range(1, n_tp):
        greet(home(lax.rem(tp + step, n_tp)))
    pl.when(has_before)(lambda: greet(beside(before)))
    pl.when(has_after)(lambda: greet(beside(after)))
    greet(facing)
    for other in planes:
        greet(level(other))

    def load(src, dst, sem):
        copy = pltpu.make_async_copy(src, dst, sem)
        copy.start()
        return copy

    def remote(src, dst, send, recv, device):
        return pltpu.make_async_remote_copy(
            src_ref=src, dst_ref=dst, send_sem=send, recv_sem=recv, device_id=device, device_id_type=MESH
        )

    block = lambda b, h: b * per + h
    order = [tp, sibling]
    for other in across:
        order += [other, other + 1 - 2 * core]

    places = [(False, r) for r in range(2 * per)] + [(True, r) for r in range(2 * per)]
    for wanted in (False, True):
        for step in range(n_y - 1):
            for h in range(per):
                places += [(wanted, (2 + 2 * step) * per + h), (wanted, (3 + 2 * step) * per + h)]

    def streams(turn):
        wanted, rank = places[turn]
        index = block(order[rank // per], rank % per)
        row = pl.multiple_of(index * width, width)
        return index, [
            pltpu.make_async_copy(ref.at[pl.ds(row, width), :], weights.at[turn % 2, i], weight_sems.at[turn % 2, i])
            for i, ref in enumerate((wo_ref,) if wanted else (wv_ref, wg_ref))
        ]

    for c in range(n_lane):
        taps_ref[c, 0:conv, :] = taps_in[:, c * LANES : (c + 1) * LANES].astype(F32)

    def gain_of(c):
        return gain_ref[:, pl.ds(pl.multiple_of(c * LANES, LANES), LANES)]

    owns = []
    for name, (hbm, vmem) in enumerate(((x_ref, xg), (g_ref, gg))):
        owns.append([
            load(hbm.at[:, pl.ds(h * width, width)], vmem.at[block(tp, h)], own_sems.at[name, h]) for h in range(per)
        ])
    for copy in streams(0)[1]:
        copy.start()

    count = n_tp - 1 + 1 + n - 1 + has_before.astype(jnp.int32) + has_after.astype(jnp.int32)
    pl.semaphore_wait(barrier, count)

    sends = Sends(send_sems)
    for hbm, vmem, recv in ((x_ref, xg, recv_x), (g_ref, gg, recv_g)):
        for h in range(per):
            src, index = hbm.at[:, pl.ds(h * width, width)], block(tp, h)
            for other in [sibling] + across:
                sends.start(src, vmem.at[index], recv.at[index], home(other))
    crossing = pl.multiple_of((1 - pair) * width, width)
    sends.start(x_ref.at[:, pl.ds(crossing, width)], px_in.at[tp], recv_px.at[tp], facing)

    part, n_part = lax.div(tp, 2), tokens // n_y

    def part_rows(index):
        start = index * n_part
        return pl.ds(start if isinstance(index, int) else pl.multiple_of(start, n_part), n_part)


    def line_send(tensor, src, b, cond):
        sends.start_if(
            jnp.logical_and(cond, b != z), src, line_in.at[tensor, z, core, part_rows(part)],
            recv_line.at[tensor, z, core, part], level(b),
        )

    column = pl.multiple_of(core * width, width)
    line_send(1, x_ref.at[part_rows(part), pl.ds(column, width)], tp, True)

    turns = iter(range(len(places)))

    def project(left):
        turn = next(turns)
        wanted, rank = places[turn]
        index, copies = streams(turn)
        if turn + 1 < len(places):
            for copy in streams(turn + 1)[1]:
                copy.start()
        for copy in copies:
            copy.wait()

        def body(j):
            cols = pl.ds(pl.multiple_of(j * 256, 256), 256)
            for i, base in enumerate((GA,) if wanted else (PV, PS)):
                value = dot(left[index], weights[turn % 2, i, :, cols])
                for side in range(2):
                    piece = value[:, side * LANES : (side + 1) * LANES]
                    if rank == 0:
                        pool[base + 2 * j + side] = piece
                    else:
                        pool[base + 2 * j + side] += piece

        loop(n_lane // 2, body)

    def land(vmem, recv, b, h):
        index = block(b, h)
        arrived(vmem.at[index], recv.at[index])
        sends.start(vmem.at[index], vmem.at[index], recv.at[index], home(sibling))

    def near(tensor, vmem, recv):
        for copy in owns[1 - tensor]:
            copy.wait()
        for h in range(per):
            project(vmem)
        for h in range(per):
            index = block(sibling, h)
            arrived(vmem.at[index], recv.at[index])
        if tensor == 1:
            line_send(1, xg.at[block(sibling, core), part_rows(part)], sibling, True)
        for h in range(per):
            project(vmem)

    def far(tensor, vmem, recv, between):
        for other in across:
            for h in range(per):
                if other is across[-1] and h == per - 1:
                    between()
                land(vmem, recv, other, h)
                line_send(tensor, vmem.at[block(other, h), part_rows(part)], other, core == h)
                if tensor == 1:
                    sends.start_if(h != pair, vmem.at[block(other, h)], px_in.at[other], recv_px.at[other], facing)
                project(vmem)
                index = block(other + 1 - 2 * core, h)
                arrived(vmem.at[index], recv.at[index])
                line_send(tensor, vmem.at[index, part_rows(part)], other + 1 - 2 * core, core == h)
                project(vmem)

    near(1, xg, recv_x)
    near(0, gg, recv_g)
    far(1, xg, recv_x, lambda: None)

    def gate(i):
        c, r = lax.div(i, tokens // ROWS), lax.rem(i, tokens // ROWS)
        rows = pl.ds(pl.multiple_of(r * ROWS, ROWS), ROWS)
        sig = sigmoid(pool[PS + c, rows, :])
        pool[PS + c, rows, :] = sig
        hp[c, pl.ds(pl.multiple_of(r * ROWS + PAD, 8), ROWS), :] = (pool[PV + c, rows, :] * sig).astype(BF16).astype(F32)

    loop(n_lane * (tokens // ROWS), gate)

    def halo(buffer, recv):
        @pl.when(jnp.logical_not(has_before))
        def _():
            buffer[:, 0:PAD, :] = jnp.zeros((n_lane, PAD, LANES), F32)

        @pl.when(jnp.logical_not(has_after))
        def _():
            buffer[:, PAD + tokens : 2 * PAD + tokens, :] = jnp.zeros((n_lane, PAD, LANES), F32)

        sends.start_if(has_after, buffer.at[:, pl.ds(tokens, PAD), :], buffer.at[:, pl.ds(0, PAD), :], recv.at[0], beside(after))
        sends.start_if(has_before, buffer.at[:, pl.ds(PAD, PAD), :], buffer.at[:, pl.ds(PAD + tokens, PAD), :], recv.at[1], beside(before))

    def halo_here(buffer, recv):
        pl.when(has_before)(lambda: arrived(buffer.at[:, pl.ds(0, PAD), :], recv.at[0]))
        pl.when(has_after)(lambda: arrived(buffer.at[:, pl.ds(PAD + tokens, PAD), :], recv.at[1]))

    halo(hp, recv_h)
    line_send(0, g_ref.at[part_rows(part), pl.ds(column, width)], tp, True)
    line_send(0, gg.at[block(sibling, core), part_rows(part)], sibling, True)

    def convolve(r):
        rows = pl.ds(pl.multiple_of(r * ROWS, ROWS), ROWS)

        def lane(c, carry):
            first, second = carry
            value = jnp.zeros((ROWS, LANES), F32)
            for k in range(conv):
                value = value + taps_ref[c, k : k + 1, :] * hp[c, pl.ds(r * ROWS + (PAD + k - radius), ROWS), :]
            pool[CV + c, rows, :] = value
            return first + value, second + value * value

        zero = jnp.zeros((ROWS, LANES), F32)
        first, second = lax.fori_loop(0, n_lane, lane, (zero, zero))
        sum_a[rows, :] = first
        sum_b[rows, :] = second

    def inner_rows(body):
        def step(r, carry):
            body(r)
            return carry

        lax.fori_loop(1, tokens // ROWS - 1, step, 0)

    inner_rows(convolve)
    halo_here(hp, recv_h)
    convolve(0)
    convolve(tokens // ROWS - 1)

    def to_row(value):
        return jnp.sum(value.T, axis=0, keepdims=True)

    def to_rows(row):
        return jnp.broadcast_to(row, (LANES, tokens)).T

    def send_sums(stat, recv):
        stat[tp, 0:1, :] = to_row(sum_a[...])
        stat[tp, 1:2, :] = to_row(sum_b[...])
        for step in range(1, n_tp):
            sends.start(stat.at[tp], stat.at[tp], recv.at[tp], home(lax.rem(tp + step, n_tp)))

    def take_sums(stat, recv):
        for step in range(1, n_tp):
            other = lax.rem(tp + step, n_tp)
            arrived(stat.at[other], recv.at[other])
        first, second = stat[0, 0:1, :], stat[0, 1:2, :]
        for other in range(1, n_tp):
            first, second = first + stat[other, 0:1, :], second + stat[other, 1:2, :]
        return first / total, second / total

    send_sums(stat1, recv_s1)

    lane_of = lambda c: pl.ds(pl.multiple_of(lax.rem(c, n_half) * LANES, LANES), LANES)

    def ag_right(k, j):
        return remote(ag.at[j, z - k], ag.at[j, z - k], ag_send.at[0, j, k], ag_recv.at[j, z - k], level(z + 1))

    def ag_left(k, j):
        return remote(ag.at[j, z + k], ag.at[j, z + k], ag_send.at[1, j, k], ag_recv.at[j, z + k], level(z - 1))

    def leave(j):
        pl.when(z < last)(lambda: ag_right(0, j).start())
        pl.when(z > 0)(lambda: ag_left(0, j).start())

    def activate():
        mean, square = take_sums(stat1, recv_s1)
        mean_b[...] = to_rows(mean)
        inv_b[...] = to_rows(lax.rsqrt(square - mean * mean + 1e-06))
        small[:, conv : conv + 1, :] = jnp.zeros((n_lane, 1, LANES), F32)

        def step(r):
            rows = pl.ds(pl.multiple_of(r * ROWS, ROWS), ROWS)
            mean_r, inv_r = mean_b[rows, :], inv_b[rows, :]

            def lane(c):
                normed = (pool[CV + c, rows, :] - mean_r) * inv_r
                pool[CV + c, rows, :] = normed
                scaled = normed * gain_of(c)
                ag[lax.div(c, n_half), z, rows, lane_of(c)] = (scaled * sigmoid(scaled)).astype(BF16)

            loop(n_lane, lane)

        loop(tokens // ROWS, step)

    far(0, gg, recv_g, activate)
    def backward(r, carry):
        rows = pl.ds(pl.multiple_of(r * ROWS, ROWS), ROWS)

        def lane(c, carry):
            first, second = carry
            normed = pool[CV + c, rows, :]
            gain = gain_of(c)
            scaled = normed * gain
            sig = sigmoid(scaled)
            grad_scaled = pool[GA + c, rows, :] * sig * (1.0 + scaled * (1.0 - sig))
            small[c, conv : conv + 1, :] += jnp.sum(grad_scaled * normed, axis=0, keepdims=True)
            grad_normed = grad_scaled * gain
            gc[c, pl.ds(pl.multiple_of(r * ROWS + PAD, 8), ROWS), :] = grad_normed
            return first + grad_normed, second + grad_normed * normed

        zero = jnp.zeros((ROWS, LANES), F32)
        first, second = lax.fori_loop(0, n_lane, lane, (zero, zero))
        sum_a[rows, :] = first
        sum_b[rows, :] = second
        return carry

    lax.fori_loop(0, tokens // ROWS, backward, 0)
    send_sums(stat2, recv_s2)

    def line_here(tensor, source, h, piece):
        ref = line_in.at[tensor, source, h, part_rows(piece)]
        arrived(ref, recv_line.at[tensor, source, h, piece])
        return ref

    def line_share(tensor):
        for source in planes:
            ref = line_here(tensor, source, core, part)
            for other in across + [sibling]:
                sends.start(ref, ref, recv_line.at[tensor, source, core, part], home(other))

    def line_pass(tensor):
        for source in planes:
            for step in range(1, n_y):
                piece = lax.rem(part + step, n_y)
                ref = line_here(tensor, source, core, piece)
                sends.start(ref, ref, recv_line.at[tensor, source, core, piece], home(sibling))

    def line_end(tensor):
        for source in planes:
            for piece in range(n_y):
                line_here(tensor, source, 1 - core, piece)

    line_share(1)
    mine = [tp] + across
    for b in mine:
        arrived(px_in.at[b], recv_px.at[b])
        sends.start(px_in.at[b], px_in.at[b], recv_px.at[b], home(sibling))
    first_mean, second_mean = take_sums(stat2, recv_s2)
    sum_a[...] = to_rows(first_mean)
    sum_b[...] = to_rows(second_mean)

    def finish(r):
        rows = pl.ds(pl.multiple_of(r * ROWS, ROWS), ROWS)
        padded = pl.ds(pl.multiple_of(r * ROWS + PAD, 8), ROWS)
        inv_r, first_r, second_r = inv_b[rows, :], sum_a[rows, :], sum_b[rows, :]

        def lane(c, carry):
            gc[c, padded, :] = inv_r * (gc[c, padded, :] - first_r - pool[CV + c, rows, :] * second_r)
            return carry

        lax.fori_loop(0, n_lane, lane, 0)

    finish(0)
    finish(tokens // ROWS - 1)
    halo(gc, recv_c)
    leave(0)
    leave(1)
    inner_rows(finish)

    def spread(r):
        rows = pl.ds(pl.multiple_of(r * ROWS, ROWS), ROWS)

        def lane(c, carry):
            value = jnp.zeros((ROWS, LANES), F32)
            for k in range(conv):
                value = value + taps_ref[c, k : k + 1, :] * gc[c, pl.ds(r * ROWS + (PAD + radius - k), ROWS), :]
            sig = pool[PS + c, rows, :]
            own_right[lax.div(c, n_half), rows, lane_of(c)] = (value * sig).astype(BF16)
            grad_gate = (value * pool[PV + c, rows, :] * sig * (1.0 - sig)).astype(BF16)

            @pl.when(c < n_half)
            def _():
                own_right[2, rows, lane_of(c)] = grad_gate

            @pl.when(c >= n_half)
            def _():
                ag[2, z, rows, lane_of(c)] = grad_gate

            return carry

        lax.fori_loop(0, n_lane, lane, 0)

    inner_rows(spread)
    halo_here(gc, recv_c)
    spread(0)
    spread(tokens // ROWS - 1)

    steps = n_tp * per

    def weight_copies(s, slot):
        b, h = lax.rem(tp + 1 + lax.div(s, per), n_tp), lax.rem(s, per)
        row = pl.multiple_of((b * per + h) * width, width)
        return [
            pltpu.make_async_copy(ref.at[pl.ds(row, width), :], weights.at[slot, i], weight_sems.at[slot, i])
            for i, ref in enumerate((wv_ref, wg_ref))
        ]

    for copy in weight_copies(0, 0):
        copy.start()
    for b in mine:
        twin = b + 1 - 2 * core
        arrived(px_in.at[twin], recv_px.at[twin])
    lefts = [load(px_in.at[d], pair_left.at[d], left_sems.at[d]) for d in range(n)]
    leave(2)
    swaps = [remote(own_right.at[j], pair_right.at[j], swap_send.at[j], swap_recv.at[j], facing) for j in range(JOBS)]
    for copy in swaps:
        copy.start()
    line_share(0)

    lead, trail = pl.ds(0, half), pl.ds(half, half)

    def input_step(s):
        slot = lax.rem(s, 2)

        @pl.when(s < steps - 1)
        def _():
            for copy in weight_copies(s + 1, 1 - slot):
                copy.start()

        for copy in weight_copies(s, slot):
            copy.wait()
        b, h = lax.rem(tp + 1 + lax.div(s, per), n_tp), lax.rem(s, per)
        value = dot_channels(own_right[0], weights[slot, 0, :, lead]) + dot_channels(own_right[1], weights[slot, 0, :, trail])
        value = value + dot_channels(own_right[2], weights[slot, 1, :, lead])
        value = (value + dot_channels(ag[2, z], weights[slot, 1, :, trail])).astype(BF16)

        @pl.when(s < steps - per)
        def _():
            gi_sent[s] = value
            remote(gi_sent.at[s], gi_in.at[tp, h], gi_send.at[s], gi_recv.at[tp, h], home(b)).start()

        @pl.when(s >= steps - per)
        def _():
            gi_own[h] = value

    loop(steps // 2, input_step)
    line_pass(1)
    for copy in lefts:
        copy.wait()
    rows = group.shape[2]

    def tap_sums(c):
        def step(r, sums):
            row = pl.multiple_of(r * 8, 8)
            grad = gc[c, pl.ds(pl.multiple_of(row + PAD, 8), 8), :]
            return tuple(sums[k] + hp[c, pl.ds(row + (PAD + k - radius), 8), :] * grad for k in range(conv))

        zeros = tuple(jnp.zeros((8, LANES), F32) for _ in range(conv))
        sums = lax.fori_loop(0, (hp.shape[1] - 2 * PAD) // 8, step, zeros)
        for k in range(conv):
            small[c, k : k + 1, :] = jnp.sum(sums[k], axis=0, keepdims=True)

    def keep(kind, j, value, add):
        for i in range(n_half):
            index, piece = (kind * JOBS + j) * n_half + i, value[:, i * LANES : (i + 1) * LANES]
            if add:
                pool[index, 0:width, :] += piece
            else:
                pool[index, 0:width, :] = piece

    def partial_rows(j, d):
        return dot_tokens(both[1, d * 2 + pair], own_right[j]) + dot_tokens(pair_left[d], pair_right[j])

    def own_rows(j):
        keep(0, j, partial_rows(j, z), False)
        tensor, cells = lax.div(j, 2), ag[j, z]
        keep(1, j, dot_tokens(both[tensor, z * 2 + pair], cells), False)
        keep(2, j, dot_tokens(both[tensor, z * 2 + 1 - pair], cells), False)

    def line_rows(j, source, side):
        tensor, cells = lax.div(j, 2), ag[j, source]
        keep(1, j, dot_tokens(line[side, tensor, pair], cells), True)
        keep(2, j, dot_tokens(line[side, tensor, 1 - pair], cells), True)

    def line_load(k, action):
        for side, (cond, source) in enumerate(((k <= z, z - k), (k <= mirror, z + k))):
            @pl.when(cond)
            def _():
                for tensor in range(2):
                    action(pltpu.make_async_copy(line_in.at[tensor, source], line.at[side, tensor], line_sems.at[side, tensor]))

    def rs_right(j, d):
        return remote(rs.at[j, d], rs.at[j, d], rs_send.at[j, d], rs_recv.at[j, d], level(z + 1))

    def rs_left(j, d):
        slot = jnp.where(d == z - 1, n, d)
        return remote(rs.at[j, d], rs.at[j, slot], rs_send.at[j, d], rs_recv.at[j, slot], level(z - 1))

    def reduce_step(j, d, waiting, copy):
        value = partial_rows(j, d)

        @pl.when(waiting)
        def _():
            arrived(rs.at[j, d], rs_recv.at[j, d])
            rs[j, d] = (value + rs[j, d].astype(F32)).astype(BF16)

        @pl.when(jnp.logical_not(waiting))
        def _():
            rs[j, d] = value.astype(BF16)

        copy(j, d).start()

    farthest = jnp.maximum(z, mirror)
    small_swap = remote(small, small_x, sx_send.at[0], sx_recv.at[0], facing)

    def add_lines(j, k):
        pl.when(k <= z)(lambda: line_rows(j, z - k, 0))
        pl.when(k <= mirror)(lambda: line_rows(j, z + k, 1))

        @pl.when(k == farthest)
        def _():
            for i in range(n_half):
                xs[j, :, i * LANES : (i + 1) * LANES] = pool[(2 * JOBS + j) * n_half + i, 0:width, :].astype(BF16)
            remote(xs.at[j], xr.at[j], xr_send.at[j], xr_recv.at[j], facing).start()

    def period(k, first):
        if not first:
            line_load(k, lambda copy: copy.start())

        def job(j):
            @pl.when(k <= z)
            def _():
                arrived(ag.at[j, z - k], ag_recv.at[j, z - k])
                pl.when(z < last)(lambda: ag_right(k, j).start())

            @pl.when(k <= mirror)
            def _():
                arrived(ag.at[j, z + k], ag_recv.at[j, z + k])
                pl.when(z > 0)(lambda: ag_left(k, j).start())

            if first:
                arrived(pair_right.at[j], swap_recv.at[j])

            @pl.when(jnp.logical_and(z < last, k > z))
            def _():
                reduce_step(j, n + z - k, z > 0, rs_right)

            @pl.when(jnp.logical_and(z > 0, k > mirror))
            def _():
                reduce_step(j, k - mirror - 1, z < last, rs_left)

            if not first:
                pl.when(j == 0)(lambda: line_load(k, lambda copy: copy.wait()))
                add_lines(j, k)

        loop(JOBS, job)

    period(1, True)
    loop(steps - steps // 2, lambda s: input_step(s + steps // 2))
    line_pass(0)
    loop(n_lane, tap_sums)
    line_end(1)
    line_end(0)
    line_load(1, lambda copy: copy.start())
    small_swap.start()
    loop(JOBS, own_rows)
    small_swap.wait_recv()
    for g in range(n):
        group[g] = (small[:, g * rows : (g + 1) * rows, :] + small_x[:, g * rows : (g + 1) * rows, :]).astype(BF16)
    group_in[z] = group[z]
    for step in range(1, n):
        other = lax.rem(z + step, n)
        remote(group.at[other], group_in.at[z], s1_send.at[step], s1_recv.at[z], level(other)).start()
    line_load(1, lambda copy: copy.wait())
    loop(JOBS, lambda j: add_lines(j, 1))

    def share_sums():
        for step in range(1, n):
            other = lax.rem(z + step, n)
            arrived(group_in.at[other], s1_recv.at[other])
        value = group_in[0].astype(F32)
        for other in range(1, n):
            value = value + group_in[other].astype(F32)
        group_all[z] = value.astype(BF16)
        for step in range(1, n):
            remote(group_all.at[z], group_all.at[z], s2_send.at[step], s2_recv.at[z], level(lax.rem(z + step, n))).start()

    def later(index):
        pl.when(index == 1)(share_sums)
        period(index + 2, False)

    loop(last - 1, later)

    loop(steps - per, lambda s: remote(gi_sent.at[s], gi_in.at[tp, 0], gi_send.at[s], gi_recv.at[tp, 0], facing).wait_send())
    arrivals = []
    for step in range(1, n_tp):
        other = lax.rem(tp + step, n_tp)
        for h in range(per):
            arrived(gi_in.at[other, h], gi_recv.at[other, h])
            slot = (step - 1) * per + h
            arrivals.append(load(gi_in.at[other, h], gi_sent.at[slot], gi_send.at[slot]))
    for copy in arrivals:
        copy.wait()
    for h in range(per):
        value = gi_own[h].astype(F32)
        for step in range(1, n_tp):
            value = value + gi_sent[(step - 1) * per + h].astype(F32)
        gi_total[:, h * width : (h + 1) * width] = value.astype(BF16)
    outs = [load(gi_total, gi_out, out_sems.at[0])]
    for step in range(1, n):
        other = lax.rem(z + step, n)
        arrived(group_all.at[other], s2_recv.at[other])
    for g in range(n):
        kept = min(rows, conv - g * rows)
        for c in range(n_lane):
            columns = slice(c * LANES, (c + 1) * LANES)
            taps_total[g * rows : g * rows + kept, columns] = group_all[g, c].astype(F32)[:kept]
            if kept < rows:
                gain_total[:, columns] = group_all[g, c].astype(F32)[kept:]
    outs.append(load(taps_total, taps_out, out_sems.at[1]))
    outs.append(load(gain_total, gain_out, out_sems.at[8]))

    def settle(kind, j, slot, into):
        for i in range(n_half):
            cols = slice(i * LANES, (i + 1) * LANES)
            value = pool[(kind * JOBS + j) * n_half + i, 0:width, :]
            for ref in slot:
                value = value + ref[:, cols].astype(F32)
            into[:, cols] = value.astype(BF16)

    for j, (ref, columns) in enumerate(((gow_out, lead), (gow_out, trail), (ggw_out, trail))):
        arrived(xr.at[j], xr_recv.at[j])
        settle(1, j, (xr.at[j],), xr.at[j])
        outs.append(load(xr.at[j], ref.at[:, columns], out_sems.at[2 + j]))
    for j, (ref, columns) in enumerate(((gvw_out, lead), (gvw_out, trail), (ggw_out, lead))):
        lower, upper = rs.at[j, z], rs.at[j, n]
        pl.when(z > 0)(lambda: arrived(lower, rs_recv.at[j, z]))
        pl.when(z < last)(lambda: arrived(upper, rs_recv.at[j, n]))
        pl.when(z == 0)(lambda: settle(0, j, (upper,), lower))
        pl.when(z == last)(lambda: settle(0, j, (lower,), lower))
        pl.when(jnp.logical_and(z > 0, z < last))(lambda: settle(0, j, (lower, upper), lower))
        outs.append(load(lower, ref.at[:, columns], out_sems.at[5 + j]))

    def sent(j):
        def step(k):
            pl.when(jnp.logical_and(k <= z, z < last))(lambda: ag_right(k, j).wait_send())
            pl.when(jnp.logical_and(k <= mirror, z > 0))(lambda: ag_left(k, j).wait_send())
            pl.when(k > z)(lambda: rs_right(j, k).wait_send())
            pl.when(k < z)(lambda: rs_left(j, k).wait_send())

        loop(n, step)
        remote(xs.at[j], xr.at[j], xr_send.at[j], xr_recv.at[j], facing).wait_send()

    loop(JOBS, sent)
    for copy in swaps + [small_swap]:
        copy.wait_send()
    sends.drain()
    for step in range(1, n):
        remote(group.at[0], group_in.at[z], s1_send.at[step], s1_recv.at[z], facing).wait_send()
        remote(group_all.at[z], group_all.at[z], s2_send.at[step], s2_recv.at[z], facing).wait_send()
    for copy in outs:
        copy.wait()


def local(inputs, w_value, w_gate, taps, ln_gain, w_out, grad_out):
    n, n_tp = lax.axis_size("outer"), lax.axis_size("tp")
    n_seq = n * 2
    tokens, own = inputs.shape
    conv, channels = taps.shape
    width = own * n_tp // n_seq
    per, n_lane, n_y, half = n_seq // n_tp, channels // LANES, n_tp // 2, channels // 2
    n_sends = (
        2 * per * n_y + 1 + 2 + 2 + 2 * 3 * (n_y - 1) * per + (n_y - 1) * per + 4 + 2 * (n_tp - 1)
        + 2 * (n - 1) * (2 * n_y - 1) + n_y
    )
    any_spec, vmem_spec = pl.BlockSpec(memory_space=pl.ANY), pl.BlockSpec(memory_space=pltpu.VMEM)
    dma = lambda *shape: pltpu.SemaphoreType.DMA(shape)
    bf, wide = (lambda *shape: pltpu.VMEM(shape, BF16)), (lambda *shape: pltpu.VMEM(shape, F32))
    out_shapes = [
        ((tokens, own), BF16), *[((width, channels), BF16)] * 3, ((conv, channels), F32), ((1, channels), F32),
        ((n_tp, tokens, width), BF16), ((2, n, 2, tokens, width), BF16), ((n_tp, per, tokens, width), BF16),
    ]
    n_gi, rows = (n_tp - 1) * per, (conv + 1) // n
    results = pl.pallas_call(
        functools.partial(kernel, n, n_tp, conv),
        name="module_backward",
        out_shape=[jax.ShapeDtypeStruct(shape, dtype) for shape, dtype in out_shapes],
        in_specs=[any_spec] * 5 + [vmem_spec] * 2,
        out_specs=[any_spec] * len(out_shapes),
        scratch_shapes=[
            wide(n_lane, conv + 1, LANES), bf(2, n_seq, tokens, width), bf(2, 2, width, channels), wide(4 * n_lane + n_lane // 2, tokens, LANES),
            wide(n_lane, tokens + 2 * PAD, LANES), wide(n_lane, tokens + 2 * PAD, LANES),
            bf(JOBS, n, tokens, half), bf(JOBS, n + 1, width, half), bf(JOBS, tokens, half), bf(JOBS, tokens, half),
            bf(n, tokens, width), bf(2, 2, 2, tokens, width),
            bf(n_gi, tokens, width), bf(per, tokens, width), bf(tokens, own),
            bf(JOBS, width, half), bf(JOBS, width, half),
            *[wide(tokens, LANES)] * 4, *[wide(n_tp, 8, tokens)] * 2,
            wide(n_lane, conv + 1, LANES), wide(n_lane, conv + 1, LANES),
            *[bf(n, n_lane, rows, LANES)] * 3, wide(conv, channels), wide(1, channels),
            dma(n_sends), dma(n_seq), dma(n_seq), dma(n_tp), dma(2, n, 2, n_y), dma(2), dma(2), dma(n_tp), dma(n_tp),
            dma(2, per), dma(2, 2), dma(n), dma(2, 2), dma(9),
            dma(2, JOBS, n), dma(JOBS, n), dma(JOBS, n + 1), dma(JOBS, n + 1), dma(JOBS), dma(JOBS), dma(JOBS), dma(JOBS),
            dma(n_gi), dma(n_tp, per),
            dma(1), dma(1), dma(n), dma(n), dma(n), dma(n),
        ],
        compiler_params=pltpu.CompilerParams(
            collective_id=0, has_side_effects=True, vmem_limit_bytes=67043328
        ),
        cost_estimate=pl.CostEstimate(
            flops=2 * 8 * tokens * width * n_seq * channels, bytes_accessed=80 * 2**20, transcendentals=0
        ),
    )(inputs, grad_out, w_value, w_gate, w_out, taps, ln_gain.reshape(1, channels))
    parts = 2
    block = lambda shape: pl.BlockSpec((shape[0] // parts, shape[1]), lambda i: (i, 0))
    fixed = lambda shape: pl.BlockSpec(shape, lambda i: (0, 0))
    shapes = [shape for shape, dtype in out_shapes[:6]]
    specs = [block(shape) for shape in shapes[:4]] + [fixed(shape) for shape in shapes[4:]]

    def write(*refs):
        for source, target in zip(refs[:6], refs[6:]):
            target[...] = source[...].astype(target.dtype)

    written = pl.pallas_call(
        write,
        name="write_results",
        grid=(parts,),
        out_shape=[jax.ShapeDtypeStruct(shape, F32 if i else BF16) for i, shape in enumerate(shapes)],
        in_specs=specs,
        out_specs=specs,
        cost_estimate=pl.CostEstimate(flops=0, bytes_accessed=11 * 2**20, transcendentals=0),
    )(*results[:6])
    return (*written[:5], written[5][0])


def solution(mesh):
    count, across = mesh.devices.shape
    fine = Mesh(mesh.devices.reshape(count // 2, 2, across), AXES)
    in_specs = (P(SP, "tp"), P(None, "tp"), P(None, "tp"), P(None, "tp"), P("tp"), P(None, "tp"), P(SP, "tp"))
    out_specs = (P(SP, "tp"), P(SP, "tp"), P(SP, "tp"), P(SP, "tp"), P(None, "tp"), P("tp"))
    return jax.shard_map(local, mesh=fine, in_specs=in_specs, out_specs=out_specs, check_vma=False)
```
